256 devices in a mesh: sp: 16 (over y, x), tp: 16 (over z, core).
Axes of the slice: x: 4, y: 4, z: 8, core: 2. Of those that a mesh axis runs over, the one named last changes fastest.
Arguments:
- query_first: bfloat16 [8192, 1536], P('sp', 'tp'), may hold values from -10 to 10
- query_second: bfloat16 [8192, 2560], P('sp', 'tp'), may hold values from -10 to 10
- latent: bfloat16 [8192, 512], P('sp'), may hold values from -400 to 400
- key_rotary: bfloat16 [8192, 32], P('sp'), may hold values from -90 to 90
- latent_gain: float32 [512], replicated, may hold values from 0.1 to 1.9
- key_up_first: bfloat16 [512, 1024], P(None, 'tp'), may hold values from -0.25 to 0.25
- value_up_first: bfloat16 [512, 1024], P(None, 'tp'), may hold values from -0.25 to 0.25
- key_up_second: bfloat16 [512, 2048], P(None, 'tp'), may hold values from -0.25 to 0.25
- value_up_second: bfloat16 [512, 2048], P(None, 'tp'), may hold values from -0.25 to 0.25
- out_first: bfloat16 [1024, 2048], P('tp'), may hold values from -0.109375 to 0.109375
- out_second: bfloat16 [2048, 2048], P('tp'), may hold values from -0.109375 to 0.109375
- residual: bfloat16 [8192, 2048], P('sp'), may hold values from -16 to 16
- expert_gain: float32 [2048], replicated, may hold values from 0.1 to 1.9
- route_experts: int32 [8192, 2], P('sp'), may hold values from 0 to 31, all different within a row; in each aligned block of 32 rows (0 to 31, 32 to 63, ...) at most 3 rows name the same one
- route_scores: float32 [8192, 2], P('sp'), may hold values from -6 to 306
- gate_weight: bfloat16 [32, 2048, 4096], P('sp', None, 'tp'), may hold values from -0.375 to 0.375
- up_weight: bfloat16 [32, 2048, 4096], P('sp', None, 'tp'), may hold values from -0.375 to 0.375
- down_weight: bfloat16 [32, 4096, 2048], P('sp', 'tp'), may hold values from -0.013671875 to 0.013671875
Outputs:
- mixed: bfloat16 [8192, 2048], P(('sp', 'tp'))
The draws below stay inside these ranges and needn't reach their ends.
Inputs may be any that keep to these rules, and one draw needn't show every extreme that they name: `route_experts`: each row names 2 different experts. In every aligned block of 32 rows no expert is named more than 3 times, and in some blocks one is named exactly 3 times.
All inputs are finite; a program needn't handle non-finite values.
Results may differ from the reference program's by a relative error of at most 0.02.
The reference program's roundings to bfloat16 on the way count: a program that leaves them out, or rounds other values in their place, can miss the bound.
Values may be sent and summed in bfloat16 or wider, within the bound.
A program may use at most 128 MiB of HBM per device.

```python
import math
import jax
import jax.numpy as jnp
import numpy as np
from jax import lax

D = 2048
HA = 16
HB = 16
NA = 64
VA = 64
NB = 128
VB = 128
ROPE = 32
RANK = 512
FF = 4096
EXPERTS = 32
TOPK = 2
CAP = 3
TOK_SP = 512
TOKENS = 8192
N_SP = 16
N_TP = 16


def scaled_field(key, rows, columns, lower, upper):
    base_key, row_key, column_key = jax.random.split(key, 3)
    base = jnp.clip(jax.random.normal(base_key, (rows, columns), jnp.float32), -4.0, 4.0)
    row_scale = jnp.exp(jax.random.uniform(row_key, (rows, 1), jnp.float32, math.log(lower), math.log(upper)))
    column_scale = jnp.exp(jax.random.uniform(column_key, (1, columns), jnp.float32, math.log(lower), math.log(upper)))
    return base * row_scale * column_scale


def draw_latent(key, part):
    return scaled_field(jax.random.fold_in(key, 11), TOKENS, RANK, 1.0, 10.0).astype(jnp.bfloat16)


def draw_residual(key, part):
    return scaled_field(jax.random.fold_in(key, 12), TOKENS, D, 0.2, 2.0).astype(jnp.bfloat16)


def draw_key_rotary(key, part):
    base_key = jax.random.fold_in(jax.random.fold_in(key, 13), 0)
    base = jnp.clip(jax.random.normal(base_key, (TOKENS, ROPE), jnp.float32), -4.0, 4.0)
    return base.astype(jnp.bfloat16)


def draw_route_scores(key, part):
    base_key = jax.random.fold_in(jax.random.fold_in(key, 14), 0)
    base = jnp.clip(1.5 * jax.random.normal(base_key, (TOKENS, TOPK), jnp.float32), -6.0, 6.0)
    return base.astype(jnp.float32)


def levels(rng, dims, pieces, least, largest):
    def one(dim, shards_of):
        draws = jax.random.uniform(jax.random.fold_in(jax.random.fold_in(rng, 6), dim), (shards_of,), jnp.float32, least / len(pieces), largest / len(pieces))
        return jnp.repeat(jnp.exp(draws), dims[dim] // shards_of).reshape((-1,) + (1,) * (len(dims) - dim - 1))

    factor_of = one(*pieces[0])
    for cut in pieces[1:]:
        factor_of = factor_of * one(*cut)
    return factor_of


def routed_block(stream_key, own, number, rows, number_of, top, bound, lean):
    sequence = jax.random.permutation(stream_key, number_of)
    crowded, ordinary = portions_of(number_of, rows * top, bound, lean, True), portions_of(number_of, rows * top, bound, lean, False)
    places = jnp.arange(number_of)

    def named(lengths, rotation):
        used = int((lengths > 0).sum())
        fixed = max(1, used // 4)
        shifted = fixed + (places - fixed + rotation * (used - fixed)) % max(1, number_of - fixed)
        return jnp.zeros((number_of,), jnp.int32).at[sequence[jnp.where(places < fixed, places, shifted)]].set(jnp.asarray(lengths, jnp.int32))

    lengths = jnp.where(number % 4 == 0, named(crowded, number // 4), named(ordinary, number - number // 4 - 1))
    mixed = jax.random.permutation(jax.random.fold_in(own, 3), number_of)
    source_of, sink = mixed[0:number_of // 2 * 2:2], mixed[1:number_of // 2 * 2:2]
    margin = jnp.minimum(lengths[source_of] - 1, bound - lengths[sink]) // 2
    margin = jnp.where((source_of == sequence[0]) | (sink == sequence[0]) | (lengths[sink] == 0), 0, jnp.maximum(margin, 0))
    shifted = jax.random.randint(jax.random.fold_in(own, 4), (number_of // 2,), 0, 1 << 20) % (margin + 1)
    lengths = lengths.at[source_of].add(-shifted).at[sink].add(shifted)
    labels = jnp.searchsorted(jnp.cumsum(lengths), jnp.arange(rows * top), side="right").astype(jnp.int32)
    grid = labels.reshape(top, rows).T
    grid = grid[jax.random.permutation(jax.random.fold_in(own, 1), rows)]
    rotation = jax.random.randint(jax.random.fold_in(own, 2), (rows, 1), 0, top)
    return jnp.take_along_axis(grid, (jnp.arange(top)[None, :] + rotation) % top, axis=1)


def portions_of(amount, total, reach, skew, full):
    loads = [(1 << 20) // math.isqrt(grade ** skew) + 1 for grade in range(1, amount + 1)]
    largest = reach if full else min(reach, max(-(-total // amount), total * loads[0] // sum(loads)))
    least = 1 if total - largest >= amount - 1 else 0
    counts, surplus = [largest] + [least] * (amount - 1), total - largest - least * (amount - 1)
    while surplus > 0:
        free = [i for i in range(1, amount) if counts[i] < largest] or [i for i in range(1, amount) if counts[i] < reach]
        mass, budget = sum([loads[i] for i in free]), surplus
        for i in free:
            addition = min(reach - counts[i], max(1, budget * loads[i] // mass), surplus)
            counts[i] = counts[i] + addition
            surplus = surplus - addition
    return np.array(counts)


def scatter_about(key, dims, scale, limit, cuts=(), kind=jnp.bfloat16):
    array = scale * jax.random.normal(key, dims, jnp.float32)
    if cuts:
        array = array * levels(key, dims, cuts, -0.22, 0.18)
    return jnp.clip(array, -limit, limit).astype(kind)


def setup_inputs(seed: int = 0) -> dict:
    key_of = jax.random.split(jax.random.key(seed), 19)
    query_first = scatter_about(key_of[0], (TOKENS, HA * (NA + ROPE)), 2.5, 10.0, ((0, 16), (1, 16)))
    query_second = scatter_about(key_of[1], (TOKENS, HB * (NB + ROPE)), 2.5, 10.0, ((0, 16), (1, 16)))
    latent = draw_latent(jax.random.fold_in(key_of[18], 71), 0)
    key_rotary = draw_key_rotary(jax.random.fold_in(key_of[18], 71), 0)
    latent_gain = jnp.clip(1.0 + 0.18 * jax.random.normal(key_of[4], (RANK,), jnp.float32), 0.1, 1.9)
    key_up_first = scatter_about(key_of[5], (RANK, HA * NA), RANK ** -0.5, 0.25, ((1, 16),))
    value_up_first = scatter_about(key_of[6], (RANK, HA * VA), RANK ** -0.5, 0.25, ((1, 16),))
    key_up_second = scatter_about(key_of[7], (RANK, HB * NB), RANK ** -0.5, 0.25, ((1, 16),))
    value_up_second = scatter_about(key_of[8], (RANK, HB * VB), RANK ** -0.5, 0.25, ((1, 16),))
    out_first = scatter_about(key_of[9], (HA * VA, D), (HA * VA + HB * VB) ** -0.5, 0.109375, ((0, 16),))
    out_second = scatter_about(key_of[10], (HB * VB, D), (HA * VA + HB * VB) ** -0.5, 0.109375, ((0, 16),))
    residual = draw_residual(jax.random.fold_in(key_of[18], 71), 0)
    expert_gain = jnp.clip(1.0 + 0.18 * jax.random.normal(key_of[12], (D,), jnp.float32), 0.1, 1.9)
    route_experts_keys = jax.random.split(jax.random.fold_in(key_of[13], 1), TOKENS // (TOK_SP // N_TP))
    route_experts_turns = jax.random.permutation(jax.random.fold_in(key_of[13], 3), TOKENS // (TOK_SP // N_TP))
    route_experts = jax.vmap(lambda own, number: routed_block(jax.random.fold_in(key_of[13], 2), own, number, TOK_SP // N_TP, EXPERTS, TOPK, CAP, 2))(route_experts_keys, route_experts_turns).reshape((TOKENS, TOPK))
    route_scores = draw_route_scores(jax.random.fold_in(key_of[18], 71), 0)
    gate_weight = scatter_about(key_of[15], (EXPERTS, D, FF), (D // 9) ** -0.5, 0.375, ((0, 16), (2, 16)))
    up_weight = scatter_about(key_of[16], (EXPERTS, D, FF), (D // 9) ** -0.5, 0.375, ((0, 16), (2, 16)))
    down_weight = scatter_about(key_of[17], (EXPERTS, FF, D), (FF * 44) ** -0.5, 0.013671875, ((0, 16), (1, 16)))
    return {"query_first": query_first, "query_second": query_second, "latent": latent, "key_rotary": key_rotary, "latent_gain": latent_gain, "key_up_first": key_up_first, "value_up_first": value_up_first, "key_up_second": key_up_second, "value_up_second": value_up_second, "out_first": out_first, "out_second": out_second, "residual": residual, "expert_gain": expert_gain, "route_experts": route_experts, "route_scores": route_scores, "gate_weight": gate_weight, "up_weight": up_weight, "down_weight": down_weight}


norm_epsilon = 1e-06
rotary_base = 10000.0
clamp_limit = 7.0
sigmoid_slope = 1.702
masked_score = -1e+30

def rotate(values, positions):
    half = values.shape[-1] // 2
    inverse = rotary_base ** (-jnp.arange(half, dtype=jnp.float32) / half)
    angles = positions.astype(jnp.float32)[:, None, None] * inverse[None, None, :]
    cosine = jnp.cos(angles)
    sine = jnp.sin(angles)
    first = values[..., :half]
    second = values[..., half:]
    return jnp.concatenate([first * cosine - second * sine, second * cosine + first * sine], axis=-1)

def rms_scaled(values, gain):
    wide = values.astype(jnp.float32)
    return wide * lax.rsqrt(lax.optimization_barrier(jnp.mean(wide * wide, axis=-1, keepdims=True)) + norm_epsilon) * gain

def turned_queries(query, nope, positions):
    shaped = query.reshape(query.shape[0], query.shape[1] // (nope + ROPE), nope + ROPE)
    turned = rotate(shaped[..., nope:].astype(jnp.float32), positions).astype(jnp.bfloat16)
    return jnp.concatenate([shaped[..., :nope], turned], axis=-1)

def clamped_unit(gate, upward):
    limited = jnp.minimum(gate, clamp_limit)
    bounded = jnp.clip(upward, -clamp_limit, clamp_limit)
    return (bounded + 1.0) * limited * jax.nn.sigmoid(sigmoid_slope * limited)

def attend_group(queries, key_nope, key_turned, values, scale):
    total = queries.shape[0]
    step_rows = math.gcd(total, 512)
    heads = queries.shape[1]
    nope = key_nope.shape[1] // heads
    keys = key_nope.reshape(total, heads, nope).astype(jnp.float32)
    value_rows = values.reshape(total, heads, values.shape[1] // heads).astype(jnp.float32)
    turned = key_turned.astype(jnp.float32)
    key_places = jnp.arange(total, dtype=jnp.int32)

    def one_block(index):
        rows = lax.dynamic_slice_in_dim(queries, index * step_rows, step_rows, 0).astype(jnp.float32)
        score = jnp.einsum('qhd,khd->qhk', rows[..., :nope], keys)
        score = (score + jnp.einsum('qhr,kr->qhk', rows[..., nope:], turned)) * scale
        places = index * step_rows + jnp.arange(step_rows, dtype=jnp.int32)
        allowed = (places[:, None] >= key_places[None, :])[:, None, :]
        score = jnp.where(allowed, score, masked_score)
        highest = lax.optimization_barrier(jnp.max(score, axis=-1, keepdims=True))
        weights = jnp.where(allowed, jnp.exp(score - highest), 0.0)
        denominator = lax.optimization_barrier(jnp.sum(weights, axis=-1))
        rounded = lax.optimization_barrier(weights.astype(jnp.bfloat16)).astype(jnp.float32)
        numerator = jnp.einsum('qhk,khd->qhd', rounded, value_rows)
        return (numerator / denominator[..., None]).astype(jnp.bfloat16)
    blocks = lax.map(one_block, jnp.arange(total // step_rows, dtype=jnp.int32))
    return blocks.reshape(total, -1)

def reference(query_first, query_second, latent, key_rotary, latent_gain, key_up_first, value_up_first, key_up_second, value_up_second, out_first, out_second, residual, expert_gain, route_experts, route_scores, gate_weight, up_weight, down_weight):
    total = latent.shape[0]
    places = jnp.arange(total, dtype=jnp.int32)
    queries_first = turned_queries(query_first, NA, places)
    queries_second = turned_queries(query_second, NB, places)
    key_turned = rotate(key_rotary.astype(jnp.float32)[:, None, :], places)[:, 0, :].astype(jnp.bfloat16)
    latent_normed = rms_scaled(latent, latent_gain).astype(jnp.bfloat16)
    key_first = jnp.dot(latent_normed, key_up_first, preferred_element_type=jnp.float32).astype(jnp.bfloat16)
    key_second = jnp.dot(latent_normed, key_up_second, preferred_element_type=jnp.float32).astype(jnp.bfloat16)
    value_first = jnp.dot(latent_normed, value_up_first, preferred_element_type=jnp.float32).astype(jnp.bfloat16)
    value_second = jnp.dot(latent_normed, value_up_second, preferred_element_type=jnp.float32).astype(jnp.bfloat16)
    attended_first = attend_group(queries_first, key_first, key_turned, value_first, (NA + ROPE) ** (-0.5))
    attended_second = attend_group(queries_second, key_second, key_turned, value_second, (NB + ROPE) ** (-0.5))
    set_first = attended_first.shape[1] // N_TP
    set_second = attended_second.shape[1] // N_TP
    projected = jnp.zeros((total, residual.shape[1]), jnp.float32)
    for index in range(N_TP):
        partial_value = jnp.dot(attended_first[:, index * set_first:(index + 1) * set_first], out_first[index * set_first:(index + 1) * set_first], preferred_element_type=jnp.float32)
        partial_value = partial_value + jnp.dot(attended_second[:, index * set_second:(index + 1) * set_second], out_second[index * set_second:(index + 1) * set_second], preferred_element_type=jnp.float32)
        projected = projected + lax.optimization_barrier(partial_value.astype(jnp.bfloat16)).astype(jnp.float32)
    middle = (residual.astype(jnp.float32) + projected).astype(jnp.bfloat16)
    normed = rms_scaled(middle, expert_gain).astype(jnp.bfloat16)
    route_weight = jax.nn.softmax(route_scores, axis=-1)
    experts = gate_weight.shape[0]
    topk = route_experts.shape[1]
    block_rows = total // (N_SP * N_TP)
    blocks = total // block_rows
    chosen = route_experts.reshape(blocks, block_rows * topk)
    hits = (chosen[..., None] == jnp.arange(experts, dtype=jnp.int32)).astype(jnp.int32)
    ranks = lax.optimization_barrier(jnp.sum((jnp.cumsum(hits, axis=1) - hits) * hits, axis=-1))
    slot_place = jnp.arange(blocks, dtype=jnp.int32)[:, None] * CAP + ranks
    owners = jnp.broadcast_to(places.reshape(blocks, block_rows, 1), (blocks, block_rows, topk)).reshape(blocks, -1)
    table = jnp.full((experts, blocks * CAP), total, jnp.int32)
    table = table.at[chosen.reshape(-1), slot_place.reshape(-1)].set(owners.reshape(-1))
    padded = jnp.concatenate([normed, jnp.zeros((1, normed.shape[1]), jnp.bfloat16)], axis=0)

    def run_expert(operands):
        slots, gate_part, up_part, down_part = operands
        rows = padded[slots]
        gate = jnp.dot(rows, gate_part, preferred_element_type=jnp.float32)
        upward = jnp.dot(rows, up_part, preferred_element_type=jnp.float32)
        activated = clamped_unit(gate, upward).astype(jnp.bfloat16)
        unit_set = activated.shape[1] // N_TP
        parts = jnp.einsum('snf,nfd->snd', activated.reshape(-1, N_TP, unit_set).astype(jnp.float32), down_part.reshape(N_TP, unit_set, -1).astype(jnp.float32))
        rounded = lax.optimization_barrier(parts.astype(jnp.bfloat16)).astype(jnp.float32)
        return lax.optimization_barrier(jnp.sum(rounded, axis=1)).astype(jnp.bfloat16)
    results = lax.map(run_expert, (table, gate_weight, up_weight, down_weight))
    picked = results[chosen.reshape(-1), slot_place.reshape(-1)].reshape(total, topk, -1).astype(jnp.float32)
    mixture = lax.optimization_barrier(jnp.sum(route_weight[..., None] * picked, axis=1))
    return (middle.astype(jnp.float32) + mixture).astype(jnp.bfloat16)
```

```python
import jax
import jax.numpy as jnp
from jax import lax
from jax.experimental import pallas as pl
from jax.experimental.pallas import tpu as pltpu
from jax.sharding import PartitionSpec as P

NA, NB, ROPE, CAP = 64, 128, 32, 3
EPS = 1e-6
MASKED = -1e30
LOG2E = 1.4426950408889634
SIDE = 4
HALF_ROWS = 256
KT_ROWS = 16
PIECE = HALF_ROWS + KT_ROWS
CUT = 144
MESH_ID = pl.DeviceIdType.MESH
STEPS = (
    (-1, 0), (1, 0), (0, -1), (0, 1), (2, 0), (-1, -1), (-1, 1), (1, -1), (1, 1),
    (0, 2), (2, -1), (2, 1), (-1, 2), (1, 2), (2, 2),
)


def pick(index, values):
    out = jnp.int32(values[0])
    for at, value in enumerate(values):
        if at:
            out = jnp.where(index == at, jnp.int32(value), out)
    return out


def attend_kernel(
    own, q1, q2, wup, of_hbm, os_hbm, res_hbm, gain,
    mid_ref, norm_ref,
    buf, wout, res, m1, l1, o1, m2, l2, o2, att, po, px, pd, rs_out, rs_in,
    g_send, g_recv, d_send, d_recv, loc_sem, x_send, x_recv, r_send, r_recv,
):
    me = lax.axis_index("sp")
    tp = lax.axis_index("tp")
    core = lax.rem(tp, 2)
    z = lax.div(tp, 2)
    y = lax.div(me, SIDE)
    x = lax.rem(me, SIDE)
    zn = lax.axis_size("tp") // 2

    def block(c, dp, dq):
        p = lax.rem(x + c * (y - x) + dp + SIDE, SIDE)
        q = lax.rem(y + c * (x - y) + dq + SIDE, SIDE)
        return p * (1 + 3 * c) + q * (4 - 3 * c)

    def sp_dev(dp, dq):
        return {"sp": block(core, dp, dq), "tp": tp}

    sib = {"sp": me, "tp": tp + 1 - 2 * core}
    z_up = {"sp": me, "tp": lax.rem(z + 1, zn) * 2 + core}
    z_dn = {"sp": me, "tp": lax.rem(z + zn - 1, zn) * 2 + core}
    peers = [sp_dev(1, 0), sp_dev(-1, 0), sp_dev(0, 1), sp_dev(0, -1), sib, z_up, z_dn]

    loads = [
        pltpu.make_async_copy(of_hbm, wout.at[pl.ds(64, 64)], loc_sem.at[0]),
        pltpu.make_async_copy(os_hbm, wout.at[pl.ds(128, 128)], loc_sem.at[1]),
        pltpu.make_async_copy(res_hbm.at[pl.ds(pl.multiple_of(tp * 32, 32), 32)], res, loc_sem.at[2]),
    ]
    for load in loads:
        load.start()
    wout[pl.ds(0, 64)] = jnp.zeros((64, wout.shape[1]), wout.dtype)

    barrier = pltpu.get_barrier_semaphore()
    for peer in peers:
        pl.semaphore_signal(barrier, inc=1, device_id=peer, device_id_type=MESH_ID)
    pl.semaphore_wait(barrier, len(peers))

    A, B, FULL = (0, CUT), (CUT, PIECE - CUT), (0, PIECE)

    def g_copy(sem, off, rows, dev, src_own=False):
        b = block(core, *off)
        src = own.at[core, pl.ds(rows[0], rows[1])] if src_own else buf.at[b, core, pl.ds(rows[0], rows[1])]
        return pltpu.make_async_remote_copy(
            src_ref=src, dst_ref=buf.at[b, core, pl.ds(rows[0], rows[1])],
            send_sem=g_send.at[sem], recv_sem=g_recv.at[sem],
            device_id=dev, device_id_type=MESH_ID,
        )

    right, left, up, down = sp_dev(1, 0), sp_dev(-1, 0), sp_dev(0, 1), sp_dev(0, -1)
    X, L, R, O = (0, 0), (-1, 0), (1, 0), (2, 0)
    sends = {
        0: (X, FULL, right, True), 1: (X, FULL, left, True), 2: (X, FULL, up, True), 3: (X, FULL, down, True),
        4: (L, A, right, False), 5: (R, B, left, False),
        6: (L, FULL, up, False), 7: (L, FULL, down, False), 8: (R, FULL, up, False), 9: (R, FULL, down, False),
        10: (O, FULL, up, False), 11: (O, FULL, down, False),
    }
    for k, dp in enumerate((0, -1, 1, 2)):
        sends[12 + 2 * k] = ((dp, -1), A, up, False)
        sends[13 + 2 * k] = ((dp, 1), B, down, False)
    arrive = {0: (L, FULL), 1: (R, FULL), 2: ((0, -1), FULL), 3: ((0, 1), FULL), 4: (O, A), 5: (O, B)}
    for k, dp in enumerate((0, -1, 1, 2)):
        if k:
            arrive[4 + 2 * k] = ((dp, -1), FULL)
            arrive[5 + 2 * k] = ((dp, 1), FULL)
        arrive[12 + 2 * k] = ((dp, 2), A)
        arrive[13 + 2 * k] = ((dp, 2), B)

    def send(sem):
        off, rows, dev, src_own = sends[sem]
        g_copy(sem, off, rows, dev, src_own).start()

    def arrived(sem):
        off, rows = arrive[sem]
        g_copy(sem, off, rows, right).wait_recv()

    def d_copy(event, blk, half):
        return pltpu.make_async_remote_copy(
            src_ref=buf.at[blk, half], dst_ref=buf.at[blk, half],
            send_sem=d_send.at[event], recv_sem=d_recv.at[event],
            device_id=sib, device_id_type=MESH_ID,
        )

    events = [
        ((0,), (4, 6, 7)), ((1,), (5, 8, 9)), ((2,), (12,)), ((3,), (13,)), ((4, 5), (10, 11)),
        ((6,), (14,)), ((7,), (15,)), ((8,), (16,)), ((9,), (17,)),
        ((12, 13), ()), ((10,), (18,)), ((11,), (19,)), ((14, 15), ()), ((16, 17), ()), ((18, 19), ()),
    ]

    for sem in (0, 1, 2, 3):
        send(sem)

    c1 = LOG2E * (NA + ROPE) ** -0.5
    c2 = LOG2E * (NB + ROPE) ** -0.5
    m1[...] = jnp.full(m1.shape, MASKED, jnp.float32)
    m2[...] = jnp.full(m2.shape, MASKED, jnp.float32)
    for ref in (l1, o1, l2, o2):
        ref[...] = jnp.zeros(ref.shape, jnp.float32)

    def unpack_turned(packed):
        wide = packed.astype(jnp.float32)
        rolled = [wide] + [pltpu.roll(wide, 512 - 32 * j, 1) for j in (1, 2, 3)]
        parts = [rolled[k % 4][:, (k // 4) * 128:(k // 4) * 128 + 128] for k in range(16)]
        return jnp.concatenate(parts, axis=0).astype(jnp.bfloat16)

    def head(q, keys, values, m, l, o, scale, masked):
        s = lax.dot_general(q[...], keys, (((1,), (1,)), ((), ())), preferred_element_type=jnp.float32)
        if masked is not None:
            s = jnp.where(masked, s, MASKED)
        old = m[...]
        new = jnp.maximum(old, jnp.max(s, axis=1, keepdims=True))
        m[...] = new
        fade = jnp.exp2((old - new) * scale)
        p = jnp.exp2((s - jnp.concatenate([new, new], axis=1)) * scale)
        l[...] = l[...] * fade + (p[:, :128] + p[:, 128:])
        o[...] = o[...] * fade + jnp.dot(p.astype(jnp.bfloat16), values, preferred_element_type=jnp.float32)

    def compute(piece, masked):
        turned = unpack_turned(piece[pl.ds(0, KT_ROWS)])
        kv = jnp.dot(piece[pl.ds(KT_ROWS, HALF_ROWS)], wup[...], preferred_element_type=jnp.float32).astype(jnp.bfloat16)
        kfv = kv[:, 128:256]
        head(q1, jnp.concatenate([kfv, turned], axis=1), kfv, m1, l1, o1, c1, masked)
        head(q2, jnp.concatenate([kv[:, :128], turned], axis=1), kv[:, 256:384], m2, l2, o2, c2, masked)

    def diag(half, _):
        rows = lax.broadcasted_iota(jnp.int32, (2 * HALF_ROWS, HALF_ROWS), 0)
        cols = lax.broadcasted_iota(jnp.int32, (2 * HALF_ROWS, HALF_ROWS), 1) + half * HALF_ROWS
        compute(own.at[half], rows >= cols)
        return 0

    lax.fori_loop(0, 2, diag, 0)

    def step(it, _):
        event = lax.div(it, 2)
        theirs = lax.rem(it, 2)
        stream = core + theirs * (1 - 2 * core)
        blk = block(stream, pick(event, [s[0] for s in STEPS]), pick(event, [s[1] for s in STEPS]))

        for number, (waits, starts) in enumerate(events):
            @pl.when(it == 2 * number)
            def _():
                for sem in waits:
                    arrived(sem)
                for sem in starts:
                    send(sem)

        @pl.when(theirs == 0)
        def _():
            d_copy(event, blk, core).start()

        @pl.when(theirs == 1)
        def _():
            d_copy(event, blk, 1 - core).wait_recv()

        @pl.when(blk < me)
        def _():
            compute(buf.at[blk, stream], None)

        return 0

    lax.fori_loop(0, 2 * len(events), step, 0)

    for sem in range(20):
        off, rows, dev, src_own = sends[sem]
        g_copy(sem, off, rows, dev, src_own).wait_send()

    def drain(event, _):
        d_copy(event, block(core, pick(event, [s[0] for s in STEPS]), pick(event, [s[1] for s in STEPS])), core).wait_send()
        return 0

    lax.fori_loop(0, len(events), drain, 0)

    a1 = o1[...] / jnp.sum(l1[...], axis=1, keepdims=True)
    a2 = o2[...] / jnp.sum(l2[...], axis=1, keepdims=True)
    lane = lax.broadcasted_iota(jnp.int32, a1.shape, 1)
    a1 = jnp.where(lane >= 64, a1, 0.0)
    both = jnp.concatenate([a1, a2], axis=1).astype(jnp.bfloat16)
    att[...] = both.reshape(att.shape)

    for load in loads:
        load.wait()

    def project(c, into):
        rows = att[:, pl.ds(c, 1)].reshape(zn * 32, 256)
        into[...] = jnp.dot(rows, wout[...], preferred_element_type=jnp.float32).astype(jnp.bfloat16).reshape(into.shape)

    def x_copy(d):
        at = lax.rem(z + d, zn)
        return pltpu.make_async_remote_copy(
            src_ref=px.at[at], dst_ref=pd.at[at], send_sem=x_send.at[d], recv_sem=x_recv.at[d],
            device_id=sib, device_id_type=MESH_ID,
        )

    far = zn // 2
    order = [far]
    for d in range(far - 1, 0, -1):
        order += [d, zn - d]
    order.append(0)
    project(1 - core, px)
    for d in order:
        x_copy(d).start()
    project(core, po)

    halves = (0, 1024)

    def pair_sum(at, col, width):
        return po[at, :, pl.ds(col, width)].astype(jnp.float32) + pd[at, :, pl.ds(col, width)].astype(jnp.float32)

    def r_copy(direction, hop, part):
        return pltpu.make_async_remote_copy(
            src_ref=rs_out.at[direction, hop, part], dst_ref=rs_in.at[direction, hop, part],
            send_sem=r_send.at[direction, hop, part], recv_sem=r_recv.at[direction, hop, part],
            device_id=z_up if direction == 0 else z_dn, device_id_type=MESH_ID,
        )

    seen = set()

    def ring(direction, hop, part):
        d = far - hop
        shift = d if direction == 0 else (zn - d) % zn
        if shift not in seen:
            x_copy(shift).wait_recv()
            seen.add(shift)
        total = pair_sum(lax.rem(z + shift, zn), halves[part], 1024)
        if hop > 0 and not (hop == 1 and part != direction):
            r_copy(direction, hop - 1, part).wait_recv()
            total = total + rs_in[direction, hop - 1, part].astype(jnp.float32)
        rs_out[direction, hop, part] = total.astype(jnp.bfloat16)
        r_copy(direction, hop, part).start()

    used = []
    for hop, flip in ((0, 0), (1, 1), (1, 0), (2, 1), (2, 0), (3, 1), (3, 0)):
        for direction in (0, 1):
            part = direction if flip == 0 else 1 - direction
            ring(direction, hop, part)
            used.append((direction, hop, part))
    x_copy(0).wait_recv()
    mids = []
    for part in (0, 1):
        total = pair_sum(z, halves[part], 1024)
        for direction in (0, 1):
            r_copy(direction, far - 1, part).wait_recv()
            total = total + rs_in[direction, far - 1, part].astype(jnp.float32)
        mids.append((res[:, pl.ds(halves[part], 1024)].astype(jnp.float32) + total).astype(jnp.bfloat16))
    mid = jnp.concatenate(mids, axis=1)
    mid_ref[...] = mid
    wide = mid.astype(jnp.float32)
    norm_ref[...] = (wide * lax.rsqrt(jnp.mean(wide * wide, axis=1, keepdims=True) + EPS) * gain[...]).astype(jnp.bfloat16)
    for d in order:
        x_copy(d).wait_send()
    for item in used:
        r_copy(*item).wait_send()


def attend(own, q1, q2, wup, out_first, out_second, residual, gain):
    vmem = pl.BlockSpec(memory_space=pltpu.VMEM)
    hbm = pl.BlockSpec(memory_space=pl.ANY)
    f32, bf16 = jnp.float32, jnp.bfloat16
    dma = pltpu.SemaphoreType.DMA
    row = pltpu.VMEM((512, 128), f32)
    return pl.pallas_call(
        attend_kernel,
        out_shape=[jax.ShapeDtypeStruct((32, 2048), bf16)] * 2,
        in_specs=[vmem, vmem, vmem, vmem, hbm, hbm, hbm, vmem],
        out_specs=[vmem, vmem],
        scratch_shapes=[
            pltpu.VMEM((16, 2, PIECE, 512), bf16),
            pltpu.VMEM((256, 2048), bf16),
            pltpu.VMEM((32, 2048), bf16),
            row, row, row, row, row, row,
            pltpu.VMEM((8, 2, 32, 256), bf16),
            pltpu.VMEM((8, 32, 2048), bf16),
            pltpu.VMEM((8, 32, 2048), bf16),
            pltpu.VMEM((8, 32, 2048), bf16),
            pltpu.VMEM((2, 4, 2, 32, 1024), bf16),
            pltpu.VMEM((2, 4, 2, 32, 1024), bf16),
            dma((20,)), dma((20,)), dma((15,)), dma((15,)), dma((3,)),
            dma((8,)), dma((8,)), dma((2, 4, 2)), dma((2, 4, 2)),
        ],
        compiler_params=pltpu.CompilerParams(collective_id=1, has_side_effects=True, vmem_limit_bytes=48 * 2**20),
        name="gather_attend",
    )(own, q1, q2, wup, out_first, out_second, residual, gain)


def rotate(values, positions):
    half = values.shape[-1] // 2
    inverse = 10000.0 ** (-jnp.arange(half, dtype=jnp.float32) / half)
    angles = positions.astype(jnp.float32)[:, None] * inverse[None, :]
    cosine = jnp.cos(angles)
    sine = jnp.sin(angles)
    first = values[:, :half]
    second = values[:, half:]
    return jnp.concatenate([first * cosine - second * sine, second * cosine + first * sine], axis=-1)


def rms_scaled(values, gain):
    wide = values.astype(jnp.float32)
    return wide * lax.rsqrt(jnp.mean(wide * wide, axis=-1, keepdims=True) + EPS) * gain


def turned(query, nope, places):
    rows = query.shape[0]
    rot = rotate(query[:, nope:].astype(jnp.float32), places).astype(jnp.bfloat16)
    pieces = [query[:, :nope]]
    if nope < 128:
        pieces.append(jnp.zeros((rows, 128 - nope), jnp.bfloat16))
    pieces += [rot, jnp.zeros((rows, 128 - ROPE), jnp.bfloat16)]
    return jnp.concatenate(pieces, axis=-1)


def attention_part(
    query_first, query_second, latent, key_rotary, latent_gain, key_up_first, value_up_first,
    key_up_second, value_up_second, out_first, out_second, residual, expert_gain,
):
    rows = latent.shape[0]
    places = lax.axis_index("sp") * rows + jnp.arange(rows, dtype=jnp.int32)
    q1 = turned(query_first, NA, places)
    q2 = turned(query_second, NB, places)
    key_turned = rotate(key_rotary.astype(jnp.float32), places).astype(jnp.bfloat16)
    normed = rms_scaled(latent, latent_gain).astype(jnp.bfloat16)
    packed = key_turned.reshape(2, 16, 16, ROPE).transpose(0, 2, 1, 3).reshape(2, KT_ROWS, 512)
    own = jnp.concatenate([packed, normed.reshape(2, HALF_ROWS, 512)], axis=1)
    wup = jnp.concatenate([key_up_second, key_up_first, value_up_first, value_up_second], axis=1)
    return attend(own, q1, q2, wup, out_first, out_second, residual, expert_gain.reshape(1, -1))


def clamped_unit(gate, upward):
    limited = jnp.minimum(gate, 7.0)
    bounded = jnp.clip(upward, -7.0, 7.0)
    return (bounded + 1.0) * limited * jax.nn.sigmoid(1.702 * limited)


def slot_numbers(chosen, experts):
    hits = (chosen[..., None] == jnp.arange(experts, dtype=jnp.int32)).astype(jnp.int32)
    before = jnp.cumsum(hits, axis=-2) - hits
    return chosen * CAP + jnp.sum(before * hits, axis=-1)


def expert_hidden(rows, gate_weight, up_weight):
    gate = jnp.einsum("nsecd,edf->nsecf", rows, gate_weight, preferred_element_type=jnp.float32)
    upward = jnp.einsum("nsecd,edf->nsecf", rows, up_weight, preferred_element_type=jnp.float32)
    return clamped_unit(gate, upward).astype(jnp.bfloat16)


def body(
    query_first, query_second, latent, key_rotary, latent_gain, key_up_first, value_up_first,
    key_up_second, value_up_second, out_first, out_second, residual, expert_gain,
    route_experts, route_scores, gate_weight, up_weight, down_weight,
):
    middle, normed = attention_part(
        query_first, query_second, latent, key_rotary, latent_gain, key_up_first, value_up_first,
        key_up_second, value_up_second, out_first, out_second, residual, expert_gain,
    )
    sets = lax.axis_size("tp")
    groups = lax.axis_size("sp")
    own_rows = latent.shape[0] // sets
    topk = route_experts.shape[1]
    local_experts = gate_weight.shape[0]
    experts = local_experts * groups
    own_start = lax.axis_index("tp") * own_rows
    slot_range = jnp.arange(experts * CAP, dtype=jnp.int32)
    own_ids = lax.dynamic_slice_in_dim(route_experts, own_start, own_rows, 0).reshape(-1)
    own_slots = slot_numbers(own_ids, experts)
    picks = (own_slots[:, None] == slot_range).reshape(own_rows, topk, experts * CAP)
    selected = jnp.sum(picks.astype(jnp.float32), axis=1).astype(jnp.bfloat16)
    outgoing = jnp.einsum("ts,td->sd", selected, normed, preferred_element_type=jnp.float32).astype(jnp.bfloat16)
    outgoing = outgoing.reshape(groups, local_experts, CAP, outgoing.shape[-1])
    arrived = lax.all_to_all(outgoing, "sp", split_axis=0, concat_axis=0, tiled=True)
    activated = expert_hidden(lax.all_gather(arrived[None], "tp", axis=0, tiled=True), gate_weight, up_weight)
    flat_hidden = activated.reshape(sets * groups, local_experts, CAP, activated.shape[-1])
    summed = lax.psum_scatter(
        jnp.einsum("secf,efd->secd", flat_hidden, down_weight, preferred_element_type=jnp.float32).astype(jnp.bfloat16),
        "tp", scatter_dimension=0, tiled=True,
    )
    returned = lax.all_to_all(summed, "sp", split_axis=0, concat_axis=0, tiled=True)
    expert_out = returned.reshape(experts * CAP, returned.shape[-1]).astype(jnp.float32)
    own_scores = lax.dynamic_slice_in_dim(route_scores, own_start, own_rows, 0)
    route_weight = jax.nn.softmax(own_scores, axis=-1)
    matches = own_slots.reshape(own_rows, topk)[..., None] == slot_range
    combine = jnp.sum(jnp.where(matches, route_weight[..., None], 0.0), axis=1)
    mixture = jnp.dot(combine, expert_out)
    return (middle.astype(jnp.float32) + mixture).astype(jnp.bfloat16)


def solution(mesh):
    in_specs = (
        P("sp", "tp"), P("sp", "tp"), P("sp", None), P("sp", None), P(),
        P(None, "tp"), P(None, "tp"), P(None, "tp"), P(None, "tp"),
        P("tp", None), P("tp", None), P("sp", None), P(),
        P("sp", None), P("sp", None), P("sp", None, "tp"), P("sp", None, "tp"), P("sp", "tp", None),
    )
    out_specs = P(("sp", "tp"), None)
    return jax.shard_map(body, mesh=mesh, in_specs=in_specs, out_specs=out_specs, check_vma=False)
```

```python
import jax
import jax.numpy as jnp
import numpy as np
from jax import lax
from jax.experimental import pallas as pl
from jax.experimental.pallas import tpu as pltpu
from jax.sharding import PartitionSpec as P

NA, NB, ROPE, CAP = 64, 128, 32, 3
EPS = 1e-6
MASKED = -1e30
LOG2E = 1.4426950408889634
SIDE = 4
HALF_ROWS = 256
KT_ROWS = 16
PIECE = HALF_ROWS + KT_ROWS
CUT = 144
MESH_ID = pl.DeviceIdType.MESH
STEPS = (
    (-1, 0), (1, 0), (0, -1), (0, 1), (2, 0), (-1, -1), (-1, 1), (1, -1), (1, 1),
    (0, 2), (2, -1), (2, 1), (-1, 2), (1, 2), (2, 2),
)


def pick(index, values):
    out = jnp.int32(values[0])
    for at, value in enumerate(values):
        if at:
            out = jnp.where(index == at, jnp.int32(value), out)
    return out


def attend_kernel(
    qf_hbm, qs_hbm, lat_hbm, kr_hbm, latg_hbm, kuf_hbm, vuf_hbm, kus_hbm, vus_hbm,
    of_hbm, os_hbm, res_hbm, gain_hbm, ids_hbm, scores_hbm, base_hbm, start_hbm,
    mid_ref, out_ref, mix_ref,
    qf, qs, lat, kr, latg, kuf, vuf, kus, vus, gain, ids, scores, base, start,
    own, q1, q2, wup,
    buf, wout, res, m1, l1, o1, m2, l2, o2, att, po, px, pd, rs_out, rs_in,
    g_send, g_recv, d_send, d_recv, loc_sem, x_send, x_recv, r_send, r_recv,
):
    me = lax.axis_index("sp")
    tp = lax.axis_index("tp")
    core = lax.rem(tp, 2)
    z = lax.div(tp, 2)
    y = lax.div(me, SIDE)
    x = lax.rem(me, SIDE)
    zn = lax.axis_size("tp") // 2

    def block(c, dp, dq):
        p = lax.rem(x + c * (y - x) + dp + SIDE, SIDE)
        q = lax.rem(y + c * (x - y) + dq + SIDE, SIDE)
        return p * (1 + 3 * c) + q * (4 - 3 * c)

    def sp_dev(dp, dq):
        return {"sp": block(core, dp, dq), "tp": tp}

    sib = {"sp": me, "tp": tp + 1 - 2 * core}
    z_up = {"sp": me, "tp": lax.rem(z + 1, zn) * 2 + core}
    z_dn = {"sp": me, "tp": lax.rem(z + zn - 1, zn) * 2 + core}
    peers = [sp_dev(1, 0), sp_dev(-1, 0), sp_dev(0, 1), sp_dev(0, -1), sib, z_up, z_dn]

    mine = pl.ds(pl.multiple_of(tp * 32, 32), 32)
    pairs = [
        (lat_hbm, lat), (latg_hbm, latg), (kr_hbm, kr), (base_hbm, base), (start_hbm, start),
        (qf_hbm, qf), (qs_hbm, qs), (kus_hbm, kus), (kuf_hbm, kuf), (vuf_hbm, vuf), (vus_hbm, vus),
        (of_hbm, wout.at[pl.ds(64, 64)]), (os_hbm, wout.at[pl.ds(128, 128)]), (res_hbm.at[mine], res),
        (gain_hbm, gain), (ids_hbm, ids), (scores_hbm, scores),
    ]
    loads = [pltpu.make_async_copy(a, b, loc_sem.at[n]) for n, (a, b) in enumerate(pairs)]
    for load in loads:
        load.start()
    wout[pl.ds(0, 64)] = jnp.zeros((64, wout.shape[1]), wout.dtype)
    m1[...] = jnp.full(m1.shape, MASKED, jnp.float32)
    m2[...] = jnp.full(m2.shape, MASKED, jnp.float32)
    for ref in (l1, o1, l2, o2):
        ref[...] = jnp.zeros(ref.shape, jnp.float32)

    barrier = pltpu.get_barrier_semaphore()
    for peer in peers:
        pl.semaphore_signal(barrier, inc=1, device_id=peer, device_id_type=MESH_ID)

    f32, bf16 = jnp.float32, jnp.bfloat16

    def placed(rows, cols, hits):
        r = lax.broadcasted_iota(jnp.int32, (rows, cols), 0)
        c = lax.broadcasted_iota(jnp.int32, (rows, cols), 1)
        total = jnp.zeros((rows, cols), f32)
        for lo, hi, shift, sign in hits:
            total = jnp.where((r == c + shift) & (c >= lo) & (c < hi), sign, total)
        return total.astype(bf16)

    def moved(value, cols, hits):
        return lax.dot_general(
            value, placed(value.shape[0], cols, hits), (((0,), (0,)), ((), ())), preferred_element_type=f32
        )

    for load in loads[:5]:
        load.wait()
    cos_r, sin_r = base[0], base[1]
    cos_0, sin_0 = start[0, pl.ds(me, 1)], start[1, pl.ds(me, 1)]
    cosine = cos_0 * cos_r - sin_0 * sin_r
    sine = sin_0 * cos_r + cos_0 * sin_r

    def rot(value, offset):
        plain = moved(value, 128, [(0, 32, offset, 1.0)])
        crossed = moved(value, 128, [(0, 16, offset + 16, -1.0), (16, 32, offset - 16, 1.0)])
        return (plain * cosine + crossed * sine).astype(bf16)

    wide = lat[...].astype(f32)
    normed = (wide * lax.rsqrt(jnp.mean(wide * wide, axis=1, keepdims=True) + EPS) * latg[...]).astype(bf16)
    own[:, pl.ds(KT_ROWS, HALF_ROWS)] = normed.reshape(2, HALF_ROWS, 512)
    kt = rot(kr[...], 0).astype(f32)
    rolled = [kt] + [pltpu.roll(kt, 32 * j, 1) for j in (1, 2, 3)]
    for half in (0, 1):
        tiles = []
        for tile in range(4):
            total = 0.0
            for j in range(4):
                first = half * HALF_ROWS + (4 * tile + j) * 16
                total = total + rolled[j][first:first + 16]
            tiles.append(total)
        own[half, pl.ds(0, KT_ROWS)] = jnp.concatenate(tiles, axis=1).astype(bf16)
    pl.semaphore_wait(barrier, len(peers))

    A, B, FULL = (0, CUT), (CUT, PIECE - CUT), (0, PIECE)

    def g_copy(sem, off, rows, dev, src_own=False):
        b = block(core, *off)
        src = own.at[core, pl.ds(rows[0], rows[1])] if src_own else buf.at[b, core, pl.ds(rows[0], rows[1])]
        return pltpu.make_async_remote_copy(
            src_ref=src, dst_ref=buf.at[b, core, pl.ds(rows[0], rows[1])],
            send_sem=g_send.at[sem], recv_sem=g_recv.at[sem],
            device_id=dev, device_id_type=MESH_ID,
        )

    right, left, up, down = sp_dev(1, 0), sp_dev(-1, 0), sp_dev(0, 1), sp_dev(0, -1)
    X, L, R, O = (0, 0), (-1, 0), (1, 0), (2, 0)
    sends = {
        0: (X, FULL, right, True), 1: (X, FULL, left, True), 2: (X, FULL, up, True), 3: (X, FULL, down, True),
        4: (L, A, right, False), 5: (R, B, left, False),
        6: (L, FULL, up, False), 7: (L, FULL, down, False), 8: (R, FULL, up, False), 9: (R, FULL, down, False),
        10: (O, FULL, up, False), 11: (O, FULL, down, False),
    }
    for k, dp in enumerate((0, -1, 1, 2)):
        sends[12 + 2 * k] = ((dp, -1), A, up, False)
        sends[13 + 2 * k] = ((dp, 1), B, down, False)
    arrive = {0: (L, FULL), 1: (R, FULL), 2: ((0, -1), FULL), 3: ((0, 1), FULL), 4: (O, A), 5: (O, B)}
    for k, dp in enumerate((0, -1, 1, 2)):
        if k:
            arrive[4 + 2 * k] = ((dp, -1), FULL)
            arrive[5 + 2 * k] = ((dp, 1), FULL)
        arrive[12 + 2 * k] = ((dp, 2), A)
        arrive[13 + 2 * k] = ((dp, 2), B)

    def send(sem):
        off, rows, dev, src_own = sends[sem]
        g_copy(sem, off, rows, dev, src_own).start()

    def arrived(sem):
        off, rows = arrive[sem]
        g_copy(sem, off, rows, right).wait_recv()

    def d_copy(event, blk, half):
        return pltpu.make_async_remote_copy(
            src_ref=buf.at[blk, half], dst_ref=buf.at[blk, half],
            send_sem=d_send.at[event], recv_sem=d_recv.at[event],
            device_id=sib, device_id_type=MESH_ID,
        )

    events = [
        ((0,), (4, 6, 7)), ((1,), (5, 8, 9)), ((2,), (12,)), ((3,), (13,)), ((4, 5), (10, 11)),
        ((6,), (14,)), ((7,), (15,)), ((8,), (16,)), ((9,), (17,)),
        ((12, 13), ()), ((10,), (18,)), ((11,), (19,)), ((14, 15), ()), ((16, 17), ()), ((18, 19), ()),
    ]

    for sem in (0, 1, 2, 3):
        send(sem)

    c1 = LOG2E * (NA + ROPE) ** -0.5
    c2 = LOG2E * (NB + ROPE) ** -0.5
    for load in loads[5:]:
        load.wait()
    q1[:, pl.ds(0, 128)] = moved(qf[...], 128, [(0, 64, 0, 1.0)]).astype(bf16)
    q1[:, pl.ds(128, 128)] = rot(qf[...], NA)
    q2[:, pl.ds(0, 128)] = moved(qs[...], 128, [(0, 128, 0, 1.0)]).astype(bf16)
    q2[:, pl.ds(128, 128)] = rot(qs[...], NB)
    wup[:, pl.ds(0, 128)] = kus[...]
    wup[:, pl.ds(128, 128)] = (moved(kuf[...], 128, [(0, 64, 0, 1.0)]) + moved(vuf[...], 128, [(64, 128, -64, 1.0)])).astype(bf16)
    wup[:, pl.ds(256, 128)] = vus[...]

    def unpack_turned(packed):
        wide = packed.astype(jnp.float32)
        rolled = [wide] + [pltpu.roll(wide, 512 - 32 * j, 1) for j in (1, 2, 3)]
        parts = [rolled[k % 4][:, (k // 4) * 128:(k // 4) * 128 + 128] for k in range(16)]
        return jnp.concatenate(parts, axis=0).astype(jnp.bfloat16)

    def head(q, keys, values, m, l, o, scale, masked):
        s = lax.dot_general(q[...], keys, (((1,), (1,)), ((), ())), preferred_element_type=jnp.float32)
        if masked is not None:
            s = jnp.where(masked, s, MASKED)
        old = m[...]
        new = jnp.maximum(old, jnp.max(s, axis=1, keepdims=True))
        m[...] = new
        fade = jnp.exp2((old - new) * scale)
        p = jnp.exp2((s - jnp.concatenate([new, new], axis=1)) * scale)
        l[...] = l[...] * fade + (p[:, :128] + p[:, 128:])
        o[...] = o[...] * fade + jnp.dot(p.astype(jnp.bfloat16), values, preferred_element_type=jnp.float32)

    def compute(piece, masked):
        turned = unpack_turned(piece[pl.ds(0, KT_ROWS)])
        kv = jnp.dot(piece[pl.ds(KT_ROWS, HALF_ROWS)], wup[...], preferred_element_type=jnp.float32).astype(jnp.bfloat16)
        kfv = kv[:, 128:256]
        head(q1, jnp.concatenate([kfv, turned], axis=1), kfv, m1, l1, o1, c1, masked)
        head(q2, jnp.concatenate([kv[:, :128], turned], axis=1), kv[:, 256:384], m2, l2, o2, c2, masked)

    def diag(half, _):
        rows = lax.broadcasted_iota(jnp.int32, (2 * HALF_ROWS, HALF_ROWS), 0)
        cols = lax.broadcasted_iota(jnp.int32, (2 * HALF_ROWS, HALF_ROWS), 1) + half * HALF_ROWS
        compute(own.at[half], rows >= cols)
        return 0

    lax.fori_loop(0, 2, diag, 0)

    count = len(events)

    def step(it, _):
        theirs = lax.rem(it, 2)
        event = lax.div(it, 2) - theirs
        stream = core + theirs * (1 - 2 * core)
        blk = block(stream, pick(event, [s[0] for s in STEPS]), pick(event, [s[1] for s in STEPS]))

        for number, (waits, starts) in enumerate(events):
            @pl.when(it == 2 * number)
            def _():
                for sem in waits:
                    arrived(sem)
                for sem in starts:
                    send(sem)

        @pl.when((theirs == 0) & (event < count))
        def _():
            d_copy(event, blk, core).start()

        @pl.when((theirs == 1) & (event >= 0))
        def _():
            d_copy(event, blk, 1 - core).wait_recv()

        @pl.when((blk < me) & (event >= 0) & (event < count))
        def _():
            compute(buf.at[blk, stream], None)

        return 0

    lax.fori_loop(0, 2 * count + 2, step, 0)

    for sem in range(20):
        off, rows, dev, src_own = sends[sem]
        g_copy(sem, off, rows, dev, src_own).wait_send()

    def drain(event, _):
        d_copy(event, block(core, pick(event, [s[0] for s in STEPS]), pick(event, [s[1] for s in STEPS])), core).wait_send()
        return 0

    lax.fori_loop(0, count, drain, 0)

    a1 = o1[...] / jnp.sum(l1[...], axis=1, keepdims=True)
    a2 = o2[...] / jnp.sum(l2[...], axis=1, keepdims=True)
    lane = lax.broadcasted_iota(jnp.int32, a1.shape, 1)
    a1 = jnp.where(lane >= 64, a1, 0.0)
    both = jnp.concatenate([a1, a2], axis=1).astype(jnp.bfloat16)
    att[...] = both.reshape(att.shape)


    def project(c, into):
        rows = att[:, pl.ds(c, 1)].reshape(zn * 32, 256)
        into[...] = jnp.dot(rows, wout[...], preferred_element_type=jnp.float32).astype(jnp.bfloat16).reshape(into.shape)

    def x_copy(d):
        at = lax.rem(z + d, zn)
        return pltpu.make_async_remote_copy(
            src_ref=px.at[at], dst_ref=pd.at[at], send_sem=x_send.at[d], recv_sem=x_recv.at[d],
            device_id=sib, device_id_type=MESH_ID,
        )

    far = zn // 2
    order = [far]
    for d in range(far - 1, 0, -1):
        order += [d, zn - d]
    order.append(0)
    project(1 - core, px)
    for d in order:
        x_copy(d).start()
    project(core, po)

    halves = (0, 1024)

    def pair_sum(at, col, width):
        return po[at, :, pl.ds(col, width)].astype(jnp.float32) + pd[at, :, pl.ds(col, width)].astype(jnp.float32)

    def r_copy(direction, hop, part):
        return pltpu.make_async_remote_copy(
            src_ref=rs_out.at[direction, hop, part], dst_ref=rs_in.at[direction, hop, part],
            send_sem=r_send.at[direction, hop, part], recv_sem=r_recv.at[direction, hop, part],
            device_id=z_up if direction == 0 else z_dn, device_id_type=MESH_ID,
        )

    seen = set()

    def ring(direction, hop, part):
        d = far - hop
        shift = d if direction == 0 else (zn - d) % zn
        if shift not in seen:
            x_copy(shift).wait_recv()
            seen.add(shift)
        total = pair_sum(lax.rem(z + shift, zn), halves[part], 1024)
        if hop > 0 and not (hop == 1 and part != direction):
            r_copy(direction, hop - 1, part).wait_recv()
            total = total + rs_in[direction, hop - 1, part].astype(jnp.float32)
        rs_out[direction, hop, part] = total.astype(jnp.bfloat16)
        r_copy(direction, hop, part).start()

    used = []
    for hop, flip in ((0, 0), (1, 1), (1, 0), (2, 1), (2, 0), (3, 1), (3, 0)):
        for direction in (0, 1):
            part = direction if flip == 0 else 1 - direction
            ring(direction, hop, part)
            used.append((direction, hop, part))
    x_copy(0).wait_recv()
    mids = []
    for part in (0, 1):
        total = pair_sum(z, halves[part], 1024)
        for direction in (0, 1):
            r_copy(direction, far - 1, part).wait_recv()
            total = total + rs_in[direction, far - 1, part].astype(jnp.float32)
        mids.append((res[:, pl.ds(halves[part], 1024)].astype(jnp.float32) + total).astype(jnp.bfloat16))
    mid = jnp.concatenate(mids, axis=1)
    mid_ref[...] = mid
    wide = mid.astype(jnp.float32)
    normed = (wide * lax.rsqrt(jnp.mean(wide * wide, axis=1, keepdims=True) + EPS) * gain[...]).astype(bf16)
    slots = out_ref.shape[0]
    token = lax.broadcasted_iota(jnp.int32, (32, 512), 1) == lax.broadcasted_iota(jnp.int32, (32, 512), 0) + tp * 32
    names = [jnp.sum(jnp.where(token, ids[k:k + 1], 0), axis=1, keepdims=True) for k in (0, 1)]
    logits = [jnp.sum(jnp.where(token, scores[k:k + 1], 0.0), axis=1, keepdims=True) for k in (0, 1)]
    hits = [(lax.broadcasted_iota(jnp.int32, (32, 128), 1) == name).astype(f32) for name in names]
    earlier = lax.broadcasted_iota(jnp.int32, (32, 32), 0) > lax.broadcasted_iota(jnp.int32, (32, 32), 1)
    before = jnp.dot(earlier.astype(bf16), (hits[0] + hits[1]).astype(bf16), preferred_element_type=f32)
    top = jnp.maximum(logits[0], logits[1])
    powers = [jnp.exp(logit - top) for logit in logits]
    picked, mix = 0.0, 0.0
    for k in (0, 1):
        rank = jnp.sum(before * hits[k], axis=1, keepdims=True)
        slot = names[k] * CAP + rank.astype(jnp.int32)
        here = (lax.broadcasted_iota(jnp.int32, (32, slots), 1) == slot).astype(f32)
        picked = picked + here
        mix = mix + here * (powers[k] / (powers[0] + powers[1]))
    mix_ref[...] = mix
    out_ref[...] = lax.dot_general(
        picked.astype(bf16), normed, (((0,), (0,)), ((), ())), preferred_element_type=f32
    ).astype(bf16)
    for d in order:
        x_copy(d).wait_send()
    for item in used:
        r_copy(*item).wait_send()


def attend(*args):
    hbm = pl.BlockSpec(memory_space=pltpu.HBM)
    vmem = pl.BlockSpec(memory_space=pltpu.VMEM)
    f32, bf16 = jnp.float32, jnp.bfloat16
    dma = pltpu.SemaphoreType.DMA
    row = pltpu.VMEM((512, 128), f32)
    place = np.arange(512)[:, None]
    first = np.arange(16)[:, None] * 512
    lanes = np.arange(128)[None, :]
    speed = 10000.0 ** (-(lanes % 16) / 16.0)
    live = lanes < ROPE
    base = np.stack([np.cos(place * speed) * live, np.sin(place * speed) * live]).astype(np.float32)
    start = np.stack([np.cos(first * speed) * live, np.sin(first * speed) * live]).astype(np.float32)
    return pl.pallas_call(
        attend_kernel,
        out_shape=[
            jax.ShapeDtypeStruct((32, 2048), bf16), jax.ShapeDtypeStruct((96, 2048), bf16),
            jax.ShapeDtypeStruct((32, 96), f32),
        ],
        in_specs=[hbm] * 17,
        out_specs=[vmem] * 3,
        scratch_shapes=[
            pltpu.VMEM((96, 512), bf16), pltpu.VMEM((160, 512), bf16), pltpu.VMEM((512, 512), bf16),
            pltpu.VMEM((32, 512), bf16), pltpu.VMEM((1, 512), f32),
            pltpu.VMEM((64, 512), bf16), pltpu.VMEM((64, 512), bf16),
            pltpu.VMEM((512, 128), bf16), pltpu.VMEM((512, 128), bf16), pltpu.VMEM((1, 2048), f32),
            pltpu.VMEM((2, 512), jnp.int32), pltpu.VMEM((2, 512), f32),
            pltpu.VMEM((2, 512, 128), f32), pltpu.VMEM((2, 16, 128), f32),
            pltpu.VMEM((2, PIECE, 512), bf16), pltpu.VMEM((512, 256), bf16), pltpu.VMEM((512, 256), bf16),
            pltpu.VMEM((512, 384), bf16),
            pltpu.VMEM((16, 2, PIECE, 512), bf16),
            pltpu.VMEM((256, 2048), bf16),
            pltpu.VMEM((32, 2048), bf16),
            row, row, row, row, row, row,
            pltpu.VMEM((8, 2, 32, 256), bf16),
            pltpu.VMEM((8, 32, 2048), bf16),
            pltpu.VMEM((8, 32, 2048), bf16),
            pltpu.VMEM((8, 32, 2048), bf16),
            pltpu.VMEM((2, 4, 2, 32, 1024), bf16),
            pltpu.VMEM((2, 4, 2, 32, 1024), bf16),
            dma((20,)), dma((20,)), dma((15,)), dma((15,)), dma((17,)),
            dma((8,)), dma((8,)), dma((2, 4, 2)), dma((2, 4, 2)),
        ],
        compiler_params=pltpu.CompilerParams(collective_id=1, has_side_effects=True, vmem_limit_bytes=67043328),
        name="gather_attend",
    )(*args, jnp.asarray(base), jnp.asarray(start))


def expert_kernel(
    own, gate_hbm, up_hbm, down_hbm, out_ref,
    gx, py, pd, wgu, wdn, rs_out, rs_in,
    w_sem, g_send, g_recv, s_send, s_recv, x_send, x_recv, r_send, r_recv,
):
    me = lax.axis_index("sp")
    tp = lax.axis_index("tp")
    core = lax.rem(tp, 2)
    z = lax.div(tp, 2)
    zn = lax.axis_size("tp") // 2
    far = zn // 2
    sib = {"sp": me, "tp": tp + 1 - 2 * core}
    z_up = {"sp": me, "tp": lax.rem(z + 1, zn) * 2 + core}
    z_dn = {"sp": me, "tp": lax.rem(z + zn - 1, zn) * 2 + core}
    peers = [sib, z_up, z_dn]

    loads = [
        pltpu.make_async_copy(gate_hbm, wgu.at[:, :, pl.ds(0, 256)], w_sem.at[0]),
        pltpu.make_async_copy(up_hbm, wgu.at[:, :, pl.ds(256, 256)], w_sem.at[1]),
        pltpu.make_async_copy(down_hbm, wdn, w_sem.at[2]),
        pltpu.make_async_copy(own, gx.at[z, core], w_sem.at[3]),
    ]
    for load in loads:
        load.start()
    barrier = pltpu.get_barrier_semaphore()
    for peer in peers:
        pl.semaphore_signal(barrier, inc=1, device_id=peer, device_id_type=MESH_ID)
    pl.semaphore_wait(barrier, len(peers))

    def at(shift):
        return lax.rem(z + shift + zn, zn)

    def g_copy(direction, hop, e):
        chip = at(-hop if direction == 0 else hop)
        return pltpu.make_async_remote_copy(
            src_ref=own.at[e] if hop == 0 else gx.at[chip, core, e],
            dst_ref=gx.at[chip, core, e],
            send_sem=g_send.at[direction, hop, e], recv_sem=g_recv.at[direction, hop, e],
            device_id=z_up if direction == 0 else z_dn, device_id_type=MESH_ID,
        )

    def g_wait(direction, hop, e):
        chip = at(-hop if direction == 0 else hop)
        pltpu.make_async_remote_copy(
            src_ref=gx.at[chip, core, e], dst_ref=gx.at[chip, core, e],
            send_sem=g_send.at[direction, hop - 1, e], recv_sem=g_recv.at[direction, hop - 1, e],
            device_id=z_up, device_id_type=MESH_ID,
        ).wait_recv()

    def s_copy(shift, e, mine):
        chip = at(shift)
        half = core if mine else 1 - core
        slot = (shift + zn) % zn
        return pltpu.make_async_remote_copy(
            src_ref=own.at[e] if shift == 0 and mine else gx.at[chip, half, e], dst_ref=gx.at[chip, half, e],
            send_sem=s_send.at[slot, e], recv_sem=s_recv.at[slot, e],
            device_id=sib, device_id_type=MESH_ID,
        )

    def x_copy(shift, e):
        chip = at(shift)
        slot = (shift + zn) % zn
        return pltpu.make_async_remote_copy(
            src_ref=py.at[1 - core, chip, e], dst_ref=pd.at[chip, e],
            send_sem=x_send.at[slot, e], recv_sem=x_recv.at[slot, e],
            device_id=sib, device_id_type=MESH_ID,
        )

    for e in (0, 1):
        for direction in (0, 1):
            g_copy(direction, 0, e).start()
    for e in (0, 1):
        s_copy(0, e, True).start()

    def compute(shifts):
        chips = [at(shift) for shift in shifts]

        def one(e, _):
            rows = jnp.concatenate([gx[chip, half, e] for chip in chips for half in (0, 1)], axis=0)
            hidden = jnp.dot(rows, wgu[e], preferred_element_type=jnp.float32)
            gate = jnp.minimum(hidden[:, :256], 7.0)
            up = jnp.clip(hidden[:, 256:], -7.0, 7.0)
            act = ((up + 1.0) * gate * (1.0 / (1.0 + jnp.exp(-1.702 * gate)))).astype(jnp.bfloat16)
            part = jnp.dot(act, wdn[e], preferred_element_type=jnp.float32).astype(jnp.bfloat16)
            for number, chip in enumerate(chips):
                for half in (0, 1):
                    py[half, chip, e] = part[(2 * number + half) * 48:(2 * number + half) * 48 + 48]
            return 0

        lax.fori_loop(0, 2, one, 0)
        for shift in shifts:
            for e in (0, 1):
                x_copy(shift, e).start()

    for load in loads:
        load.wait()
    for e in (0, 1):
        s_copy(0, e, False).wait_recv()
    compute([0])

    for hop in range(1, far + 1):
        for e in (0, 1):
            for direction in (0, 1):
                if hop == far and e != direction:
                    continue
                g_wait(direction, hop, e)
                if hop < far - 1 or (hop == far - 1 and e == direction):
                    g_copy(direction, hop, e).start()
                s_copy(-hop if direction == 0 else hop, e, True).start()
        shifts = [-hop, hop] if hop < far else [far]
        for shift in shifts:
            for e in (0, 1):
                s_copy(shift, e, False).wait_recv()
        compute(shifts)

    def pair_sum(shift, e):
        chip = at(shift)
        return py[core, chip, e].astype(jnp.float32) + pd[chip, e].astype(jnp.float32)

    def r_copy(direction, hop, e):
        return pltpu.make_async_remote_copy(
            src_ref=rs_out.at[direction, hop, e], dst_ref=rs_in.at[direction, hop, e],
            send_sem=r_send.at[direction, hop, e], recv_sem=r_recv.at[direction, hop, e],
            device_id=z_up if direction == 0 else z_dn, device_id_type=MESH_ID,
        )

    seen = set()
    used = []
    for hop, flip in ((0, 0), (1, 1), (1, 0), (2, 1), (2, 0), (3, 1), (3, 0)):
        for direction in (0, 1):
            e = direction if flip == 0 else 1 - direction
            shift = (far - hop) if direction == 0 else -(far - hop)
            key = (shift % zn, e)
            if key not in seen:
                seen.add(key)
                x_copy(shift, e).wait_recv()
            total = pair_sum(shift, e)
            if hop > 0 and not (hop == 1 and e != direction):
                r_copy(direction, hop - 1, e).wait_recv()
                total = total + rs_in[direction, hop - 1, e].astype(jnp.float32)
            rs_out[direction, hop, e] = total.astype(jnp.bfloat16)
            r_copy(direction, hop, e).start()
            used.append((direction, hop, e))
    for e in (0, 1):
        x_copy(0, e).wait_recv()
        total = pair_sum(0, e)
        for direction in (0, 1):
            r_copy(direction, far - 1, e).wait_recv()
            total = total + rs_in[direction, far - 1, e].astype(jnp.float32)
        out_ref[e] = total.astype(jnp.bfloat16)

    for item in used:
        r_copy(*item).wait_send()
    for e in (0, 1):
        for shift in range(-far + 1, far + 1):
            s_copy(shift, e, True).wait_send()
            x_copy(shift, e).wait_send()
        for direction in (0, 1):
            for hop in range(far):
                if hop < far - 1 or e == direction:
                    g_copy(direction, hop, e).wait_send()


def run_experts(rows, gate_weight, up_weight, down_weight):
    vmem = pl.BlockSpec(memory_space=pltpu.VMEM)
    hbm = pl.BlockSpec(memory_space=pl.ANY)
    bf16 = jnp.bfloat16
    dma = pltpu.SemaphoreType.DMA
    return pl.pallas_call(
        expert_kernel,
        out_shape=jax.ShapeDtypeStruct((2, 48, 2048), bf16),
        in_specs=[vmem, hbm, hbm, hbm],
        out_specs=vmem,
        scratch_shapes=[
            pltpu.VMEM((8, 2, 2, 48, 2048), bf16),
            pltpu.VMEM((2, 8, 2, 48, 2048), bf16),
            pltpu.VMEM((8, 2, 48, 2048), bf16),
            pltpu.VMEM((2, 2048, 512), bf16),
            pltpu.VMEM((2, 256, 2048), bf16),
            pltpu.VMEM((2, 4, 2, 48, 2048), bf16),
            pltpu.VMEM((2, 4, 2, 48, 2048), bf16),
            dma((4,)), dma((2, 4, 2)), dma((2, 4, 2)), dma((8, 2)), dma((8, 2)),
            dma((8, 2)), dma((8, 2)), dma((2, 4, 2)), dma((2, 4, 2)),
        ],
        compiler_params=pltpu.CompilerParams(collective_id=2, has_side_effects=True, vmem_limit_bytes=56 * 2**20),
        name="experts",
    )(rows, gate_weight, up_weight, down_weight)


def body(
    query_first, query_second, latent, key_rotary, latent_gain, key_up_first, value_up_first,
    key_up_second, value_up_second, out_first, out_second, residual, expert_gain,
    route_experts, route_scores, gate_weight, up_weight, down_weight,
):
    middle, outgoing, mix = attend(
        query_first.T, query_second.T, latent, key_rotary.T, latent_gain.reshape(1, -1), key_up_first.T, value_up_first.T,
        key_up_second, value_up_second, out_first, out_second, residual, expert_gain.reshape(1, -1),
        route_experts.T, route_scores.T,
    )
    groups = lax.axis_size("sp")
    local_experts = gate_weight.shape[0]
    outgoing = outgoing.reshape(groups, local_experts, CAP, outgoing.shape[-1])
    arrived = lax.all_to_all(outgoing, "sp", split_axis=0, concat_axis=0, tiled=True)
    rows = arrived.transpose(1, 0, 2, 3).reshape(local_experts, groups * CAP, -1)
    summed = run_experts(rows, gate_weight, up_weight, down_weight)
    summed = summed.reshape(local_experts, groups, CAP, -1).transpose(1, 0, 2, 3)
    returned = lax.all_to_all(summed, "sp", split_axis=0, concat_axis=0, tiled=True)
    expert_out = returned.reshape(groups * local_experts * CAP, returned.shape[-1]).astype(jnp.float32)
    mixture = jnp.dot(mix, expert_out)
    return (middle.astype(jnp.float32) + mixture).astype(jnp.bfloat16)


def solution(mesh):
    in_specs = (
        P("sp", "tp"), P("sp", "tp"), P("sp", None), P("sp", None), P(),
        P(None, "tp"), P(None, "tp"), P(None, "tp"), P(None, "tp"),
        P("tp", None), P("tp", None), P("sp", None), P(),
        P("sp", None), P("sp", None), P("sp", None, "tp"), P("sp", None, "tp"), P("sp", "tp", None),
    )
    out_specs = P(("sp", "tp"), None)
    return jax.shard_map(body, mesh=mesh, in_specs=in_specs, out_specs=out_specs, check_vma=False)
```

```python
import jax
import jax.numpy as jnp
import numpy as np
from jax import lax
from jax.experimental import pallas as pl
from jax.experimental.pallas import tpu as pltpu
from jax.sharding import PartitionSpec as P

NA, NB, ROPE, CAP = 64, 128, 32, 3
EPS = 1e-6
MASKED = -1e30
LOG2E = 1.4426950408889634
SIDE = 4
HALF_ROWS = 256
KT_ROWS = 16
PIECE = HALF_ROWS + KT_ROWS
A_SCRATCH = 42
CUT = 144
MESH_ID = pl.DeviceIdType.MESH
STEPS = (
    (-1, 0), (1, 0), (0, -1), (0, 1), (2, 0), (-1, -1), (-1, 1), (1, -1), (1, 1),
    (0, 2), (2, -1), (2, 1), (-1, 2), (1, 2), (2, 2),
)


def pick(index, values):
    out = jnp.int32(values[0])
    for at, value in enumerate(values):
        if at:
            out = jnp.where(index == at, jnp.int32(value), out)
    return out


def attend_kernel(
    weight_loads, qf_hbm, qs_hbm, lat_hbm, kr_hbm, latg_hbm, kuf_hbm, vuf_hbm, kus_hbm, vus_hbm,
    of_hbm, os_hbm, res_hbm, gain_hbm, ids_hbm, scores_hbm, base_hbm, start_hbm,
    mid_ref, out_ref, mix_ref,
    qf, qs, lat, kr, latg, kuf, vuf, kus, vus, gain, ids, scores, base, start,
    own, q1, q2, wup,
    buf, wout, res, m1, l1, o1, m2, l2, o2, att, po, px, pd, rs_out, rs_in,
    g_send, g_recv, d_send, d_recv, loc_sem, x_send, x_recv, r_send, r_recv,
):
    me = lax.axis_index("sp")
    tp = lax.axis_index("tp")
    core = lax.rem(tp, 2)
    z = lax.div(tp, 2)
    y = lax.div(me, SIDE)
    x = lax.rem(me, SIDE)
    zn = lax.axis_size("tp") // 2

    def block(c, dp, dq):
        p = lax.rem(x + c * (y - x) + dp + SIDE, SIDE)
        q = lax.rem(y + c * (x - y) + dq + SIDE, SIDE)
        return p * (1 + 3 * c) + q * (4 - 3 * c)

    def sp_dev(dp, dq):
        return {"sp": block(core, dp, dq), "tp": tp}

    sib = {"sp": me, "tp": tp + 1 - 2 * core}
    z_up = {"sp": me, "tp": lax.rem(z + 1, zn) * 2 + core}
    z_dn = {"sp": me, "tp": lax.rem(z + zn - 1, zn) * 2 + core}
    groups = lax.axis_size("sp")
    peers = [sib, z_up, z_dn] + [{"sp": lax.rem(me + k, groups), "tp": tp} for k in range(1, groups)]

    mine = pl.ds(pl.multiple_of(tp * 32, 32), 32)
    pairs = [
        (lat_hbm, lat), (latg_hbm, latg), (kr_hbm, kr), (base_hbm, base), (start_hbm, start),
        (qf_hbm, qf), (qs_hbm, qs), (kus_hbm, kus), (kuf_hbm, kuf), (vuf_hbm, vuf), (vus_hbm, vus),
        (of_hbm, wout.at[pl.ds(64, 64)]), (os_hbm, wout.at[pl.ds(128, 128)]), (res_hbm.at[mine], res),
        (gain_hbm, gain), (ids_hbm, ids), (scores_hbm, scores),
    ]
    loads = [pltpu.make_async_copy(a, b, loc_sem.at[n]) for n, (a, b) in enumerate(pairs)]
    for load in loads + weight_loads:
        load.start()
    wout[pl.ds(0, 64)] = jnp.zeros((64, wout.shape[1]), wout.dtype)
    m1[...] = jnp.full(m1.shape, MASKED, jnp.float32)
    m2[...] = jnp.full(m2.shape, MASKED, jnp.float32)
    for ref in (l1, o1, l2, o2):
        ref[...] = jnp.zeros(ref.shape, jnp.float32)

    barrier = pltpu.get_barrier_semaphore()
    for peer in peers:
        pl.semaphore_signal(barrier, inc=1, device_id=peer, device_id_type=MESH_ID)

    f32, bf16 = jnp.float32, jnp.bfloat16

    def placed(rows, cols, hits):
        r = lax.broadcasted_iota(jnp.int32, (rows, cols), 0)
        c = lax.broadcasted_iota(jnp.int32, (rows, cols), 1)
        total = jnp.zeros((rows, cols), f32)
        for lo, hi, shift, sign in hits:
            total = jnp.where((r == c + shift) & (c >= lo) & (c < hi), sign, total)
        return total.astype(bf16)

    def moved(value, cols, hits):
        return lax.dot_general(
            value, placed(value.shape[0], cols, hits), (((0,), (0,)), ((), ())), preferred_element_type=f32
        )

    for load in loads[:5]:
        load.wait()
    cos_r, sin_r = base[0], base[1]
    cos_0, sin_0 = start[0, pl.ds(me, 1)], start[1, pl.ds(me, 1)]
    cosine = cos_0 * cos_r - sin_0 * sin_r
    sine = sin_0 * cos_r + cos_0 * sin_r

    def rot(value, offset):
        plain = moved(value, 128, [(0, 32, offset, 1.0)])
        crossed = moved(value, 128, [(0, 16, offset + 16, -1.0), (16, 32, offset - 16, 1.0)])
        return (plain * cosine + crossed * sine).astype(bf16)

    wide = lat[...].astype(f32)
    normed = (wide * lax.rsqrt(jnp.mean(wide * wide, axis=1, keepdims=True) + EPS) * latg[...]).astype(bf16)
    own[:, pl.ds(KT_ROWS, HALF_ROWS)] = normed.reshape(2, HALF_ROWS, 512)
    kt = rot(kr[...], 0).astype(f32)
    rolled = [kt] + [pltpu.roll(kt, 32 * j, 1) for j in (1, 2, 3)]
    for half in (0, 1):
        tiles = []
        for tile in range(4):
            total = 0.0
            for j in range(4):
                first = half * HALF_ROWS + (4 * tile + j) * 16
                total = total + rolled[j][first:first + 16]
            tiles.append(total)
        own[half, pl.ds(0, KT_ROWS)] = jnp.concatenate(tiles, axis=1).astype(bf16)
    pl.semaphore_wait(barrier, len(peers))

    A, B, FULL = (0, CUT), (CUT, PIECE - CUT), (0, PIECE)

    def g_copy(sem, off, rows, dev, src_own=False):
        b = block(core, *off)
        src = own.at[core, pl.ds(rows[0], rows[1])] if src_own else buf.at[b, core, pl.ds(rows[0], rows[1])]
        return pltpu.make_async_remote_copy(
            src_ref=src, dst_ref=buf.at[b, core, pl.ds(rows[0], rows[1])],
            send_sem=g_send.at[sem], recv_sem=g_recv.at[sem],
            device_id=dev, device_id_type=MESH_ID,
        )

    right, left, up, down = sp_dev(1, 0), sp_dev(-1, 0), sp_dev(0, 1), sp_dev(0, -1)
    X, L, R, O = (0, 0), (-1, 0), (1, 0), (2, 0)
    sends = {
        0: (X, FULL, right, True), 1: (X, FULL, left, True), 2: (X, FULL, up, True), 3: (X, FULL, down, True),
        4: (L, A, right, False), 5: (R, B, left, False),
        6: (L, FULL, up, False), 7: (L, FULL, down, False), 8: (R, FULL, up, False), 9: (R, FULL, down, False),
        10: (O, FULL, up, False), 11: (O, FULL, down, False),
    }
    for k, dp in enumerate((0, -1, 1, 2)):
        sends[12 + 2 * k] = ((dp, -1), A, up, False)
        sends[13 + 2 * k] = ((dp, 1), B, down, False)
    arrive = {0: (L, FULL), 1: (R, FULL), 2: ((0, -1), FULL), 3: ((0, 1), FULL), 4: (O, A), 5: (O, B)}
    for k, dp in enumerate((0, -1, 1, 2)):
        if k:
            arrive[4 + 2 * k] = ((dp, -1), FULL)
            arrive[5 + 2 * k] = ((dp, 1), FULL)
        arrive[12 + 2 * k] = ((dp, 2), A)
        arrive[13 + 2 * k] = ((dp, 2), B)

    def send(sem):
        off, rows, dev, src_own = sends[sem]
        g_copy(sem, off, rows, dev, src_own).start()

    def arrived(sem):
        off, rows = arrive[sem]
        g_copy(sem, off, rows, right).wait_recv()

    def d_copy(event, blk, half):
        return pltpu.make_async_remote_copy(
            src_ref=buf.at[blk, half], dst_ref=buf.at[blk, half],
            send_sem=d_send.at[event], recv_sem=d_recv.at[event],
            device_id=sib, device_id_type=MESH_ID,
        )

    events = [
        ((0,), (4, 6, 7)), ((1,), (5, 8, 9)), ((2,), (12,)), ((3,), (13,)), ((4, 5), (10, 11)),
        ((6,), (14,)), ((7,), (15,)), ((8,), (16,)), ((9,), (17,)),
        ((12, 13), ()), ((10,), (18,)), ((11,), (19,)), ((14, 15), ()), ((16, 17), ()), ((18, 19), ()),
    ]

    for sem in (0, 1, 2, 3):
        send(sem)

    c1 = LOG2E * (NA + ROPE) ** -0.5
    c2 = LOG2E * (NB + ROPE) ** -0.5
    for load in loads[5:]:
        load.wait()
    q1[:, pl.ds(0, 128)] = moved(qf[...], 128, [(0, 64, 0, 1.0)]).astype(bf16)
    q1[:, pl.ds(128, 128)] = rot(qf[...], NA)
    q2[:, pl.ds(0, 128)] = moved(qs[...], 128, [(0, 128, 0, 1.0)]).astype(bf16)
    q2[:, pl.ds(128, 128)] = rot(qs[...], NB)
    wup[:, pl.ds(0, 128)] = kus[...]
    wup[:, pl.ds(128, 128)] = (moved(kuf[...], 128, [(0, 64, 0, 1.0)]) + moved(vuf[...], 128, [(64, 128, -64, 1.0)])).astype(bf16)
    wup[:, pl.ds(256, 128)] = vus[...]

    def unpack_turned(packed):
        wide = packed.astype(jnp.float32)
        rolled = [wide] + [pltpu.roll(wide, 512 - 32 * j, 1) for j in (1, 2, 3)]
        parts = [rolled[k % 4][:, (k // 4) * 128:(k // 4) * 128 + 128] for k in range(16)]
        return jnp.concatenate(parts, axis=0).astype(jnp.bfloat16)

    def head(q, keys, values, m, l, o, scale, masked):
        s = lax.dot_general(q[...], keys, (((1,), (1,)), ((), ())), preferred_element_type=jnp.float32)
        if masked is not None:
            s = jnp.where(masked, s, MASKED)
        old = m[...]
        new = jnp.maximum(old, jnp.max(s, axis=1, keepdims=True))
        m[...] = new
        fade = jnp.exp2((old - new) * scale)
        p = jnp.exp2((s - jnp.concatenate([new, new], axis=1)) * scale)
        l[...] = l[...] * fade + (p[:, :128] + p[:, 128:])
        o[...] = o[...] * fade + jnp.dot(p.astype(jnp.bfloat16), values, preferred_element_type=jnp.float32)

    def compute(piece, masked):
        turned = unpack_turned(piece[pl.ds(0, KT_ROWS)])
        kv = jnp.dot(piece[pl.ds(KT_ROWS, HALF_ROWS)], wup[...], preferred_element_type=jnp.float32).astype(jnp.bfloat16)
        kfv = kv[:, 128:256]
        head(q1, jnp.concatenate([kfv, turned], axis=1), kfv, m1, l1, o1, c1, masked)
        head(q2, jnp.concatenate([kv[:, :128], turned], axis=1), kv[:, 256:384], m2, l2, o2, c2, masked)

    def diag(half, _):
        rows = lax.broadcasted_iota(jnp.int32, (2 * HALF_ROWS, HALF_ROWS), 0)
        cols = lax.broadcasted_iota(jnp.int32, (2 * HALF_ROWS, HALF_ROWS), 1) + half * HALF_ROWS
        compute(own.at[half], rows >= cols)
        return 0

    lax.fori_loop(0, 2, diag, 0)

    count = len(events)

    def step(it, _):
        theirs = lax.rem(it, 2)
        event = lax.div(it, 2) - theirs
        stream = core + theirs * (1 - 2 * core)
        blk = block(stream, pick(event, [s[0] for s in STEPS]), pick(event, [s[1] for s in STEPS]))

        for number, (waits, starts) in enumerate(events):
            @pl.when(it == 2 * number)
            def _():
                for sem in waits:
                    arrived(sem)
                for sem in starts:
                    send(sem)

        @pl.when((theirs == 0) & (event < count))
        def _():
            d_copy(event, blk, core).start()

        @pl.when((theirs == 1) & (event >= 0))
        def _():
            d_copy(event, blk, 1 - core).wait_recv()

        @pl.when((blk < me) & (event >= 0) & (event < count))
        def _():
            compute(buf.at[blk, stream], None)

        return 0

    lax.fori_loop(0, 2 * count + 2, step, 0)

    for sem in range(20):
        off, rows, dev, src_own = sends[sem]
        g_copy(sem, off, rows, dev, src_own).wait_send()

    def drain(event, _):
        d_copy(event, block(core, pick(event, [s[0] for s in STEPS]), pick(event, [s[1] for s in STEPS])), core).wait_send()
        return 0

    lax.fori_loop(0, count, drain, 0)

    a1 = o1[...] / jnp.sum(l1[...], axis=1, keepdims=True)
    a2 = o2[...] / jnp.sum(l2[...], axis=1, keepdims=True)
    lane = lax.broadcasted_iota(jnp.int32, a1.shape, 1)
    a1 = jnp.where(lane >= 64, a1, 0.0)
    both = jnp.concatenate([a1, a2], axis=1).astype(jnp.bfloat16)
    att[...] = both.reshape(att.shape)


    def project(c, into):
        rows = att[:, pl.ds(c, 1)].reshape(zn * 32, 256)
        into[...] = jnp.dot(rows, wout[...], preferred_element_type=jnp.float32).astype(jnp.bfloat16).reshape(into.shape)

    def x_copy(d):
        at = lax.rem(z + d, zn)
        return pltpu.make_async_remote_copy(
            src_ref=px.at[at], dst_ref=pd.at[at], send_sem=x_send.at[d], recv_sem=x_recv.at[d],
            device_id=sib, device_id_type=MESH_ID,
        )

    far = zn // 2
    order = [far]
    for d in range(far - 1, 0, -1):
        order += [d, zn - d]
    order.append(0)
    project(1 - core, px)
    for d in order:
        x_copy(d).start()
    project(core, po)

    halves = (0, 1024)

    def pair_sum(at, col, width):
        return po[at, :, pl.ds(col, width)].astype(jnp.float32) + pd[at, :, pl.ds(col, width)].astype(jnp.float32)

    def r_copy(direction, hop, part):
        return pltpu.make_async_remote_copy(
            src_ref=rs_out.at[direction, hop, part], dst_ref=rs_in.at[direction, hop, part],
            send_sem=r_send.at[direction, hop, part], recv_sem=r_recv.at[direction, hop, part],
            device_id=z_up if direction == 0 else z_dn, device_id_type=MESH_ID,
        )

    seen = set()

    def ring(direction, hop, part):
        d = far - hop
        shift = d if direction == 0 else (zn - d) % zn
        if shift not in seen:
            x_copy(shift).wait_recv()
            seen.add(shift)
        total = pair_sum(lax.rem(z + shift, zn), halves[part], 1024)
        if hop > 0 and not (hop == 1 and part != direction):
            r_copy(direction, hop - 1, part).wait_recv()
            total = total + rs_in[direction, hop - 1, part].astype(jnp.float32)
        rs_out[direction, hop, part] = total.astype(jnp.bfloat16)
        r_copy(direction, hop, part).start()

    used = []
    for hop, flip in ((0, 0), (1, 1), (1, 0), (2, 1), (2, 0), (3, 1), (3, 0)):
        for direction in (0, 1):
            part = direction if flip == 0 else 1 - direction
            ring(direction, hop, part)
            used.append((direction, hop, part))
    x_copy(0).wait_recv()
    mids = []
    for part in (0, 1):
        total = pair_sum(z, halves[part], 1024)
        for direction in (0, 1):
            r_copy(direction, far - 1, part).wait_recv()
            total = total + rs_in[direction, far - 1, part].astype(jnp.float32)
        mids.append((res[:, pl.ds(halves[part], 1024)].astype(jnp.float32) + total).astype(jnp.bfloat16))
    mid = jnp.concatenate(mids, axis=1)
    mid_ref[...] = mid
    wide = mid.astype(jnp.float32)
    normed = (wide * lax.rsqrt(jnp.mean(wide * wide, axis=1, keepdims=True) + EPS) * gain[...]).astype(bf16)
    slots = mix_ref.shape[1]
    token = lax.broadcasted_iota(jnp.int32, (32, 512), 1) == lax.broadcasted_iota(jnp.int32, (32, 512), 0) + tp * 32
    names = [jnp.sum(jnp.where(token, ids[k:k + 1], 0), axis=1, keepdims=True) for k in (0, 1)]
    logits = [jnp.sum(jnp.where(token, scores[k:k + 1], 0.0), axis=1, keepdims=True) for k in (0, 1)]
    hits = [(lax.broadcasted_iota(jnp.int32, (32, 128), 1) == name).astype(f32) for name in names]
    earlier = lax.broadcasted_iota(jnp.int32, (32, 32), 0) > lax.broadcasted_iota(jnp.int32, (32, 32), 1)
    before = jnp.dot(earlier.astype(bf16), (hits[0] + hits[1]).astype(bf16), preferred_element_type=f32)
    top = jnp.maximum(logits[0], logits[1])
    powers = [jnp.exp(logit - top) for logit in logits]
    picked, mix = 0.0, 0.0
    for k in (0, 1):
        rank = jnp.sum(before * hits[k], axis=1, keepdims=True)
        slot = (names[k] >> 1) * 8 + (names[k] & 1) * CAP + rank.astype(jnp.int32)
        here = (lax.broadcasted_iota(jnp.int32, (32, slots), 1) == slot).astype(f32)
        picked = picked + here
        mix = mix + here * (powers[k] / (powers[0] + powers[1]))
    mix_ref[...] = mix
    out_ref[...] = lax.dot_general(
        picked.astype(bf16), normed, (((0,), (0,)), ((), ())), preferred_element_type=f32
    ).astype(bf16).reshape(out_ref.shape)
    for d in order:
        x_copy(d).wait_send()
    for item in used:
        r_copy(*item).wait_send()


def expert_kernel(
    going, mid, mix, loads, out_ref,
    a_in, b_out, b_in, own, gx, py, pd, wgu, wdn, rs_out, rs_in,
    a_send, a_recv, b_send, b_recv, g_send, g_recv, s_send, s_recv, x_send, x_recv, r_send, r_recv,
):
    me = lax.axis_index("sp")
    tp = lax.axis_index("tp")
    core = lax.rem(tp, 2)
    z = lax.div(tp, 2)
    zn = lax.axis_size("tp") // 2
    far = zn // 2
    sib = {"sp": me, "tp": tp + 1 - 2 * core}
    z_up = {"sp": me, "tp": lax.rem(z + 1, zn) * 2 + core}
    z_dn = {"sp": me, "tp": lax.rem(z + zn - 1, zn) * 2 + core}
    groups = lax.axis_size("sp")

    def exchange(k, src, dst, send_sems, recv_sems):
        peer = lax.rem(me + k, groups)
        return pltpu.make_async_remote_copy(
            src_ref=src.at[peer, pl.ds(0, 6)], dst_ref=dst.at[me, pl.ds(0, 6)], send_sem=send_sems.at[k], recv_sem=recv_sems.at[k],
            device_id={"sp": peer, "tp": tp}, device_id_type=MESH_ID,
        )

    def exchanged(k, dst, send_sems, recv_sems):
        peer = lax.rem(me + groups - k, groups)
        pltpu.make_async_remote_copy(
            src_ref=dst.at[peer, pl.ds(0, 6)], dst_ref=dst.at[peer, pl.ds(0, 6)], send_sem=send_sems.at[k], recv_sem=recv_sems.at[k],
            device_id={"sp": peer, "tp": tp}, device_id_type=MESH_ID,
        ).wait_recv()

    def each(act):
        def one(k, _):
            act(k)
            return 0

        lax.fori_loop(1, groups, one, 0)

    each(lambda k: exchange(k, going, a_in, a_send, a_recv).start())
    a_in[me] = going[me]
    row = lax.broadcasted_iota(jnp.int32, (96, 128), 0)
    col = lax.broadcasted_iota(jnp.int32, (96, 128), 1)
    inner = col & 7
    second = (inner >= CAP).astype(jnp.int32)
    wanted = second * 48 + (col >> 3) * CAP + inner - second * CAP
    compact = ((row == wanted) & (inner < 2 * CAP)).astype(jnp.float32).astype(jnp.bfloat16)
    each(lambda k: exchanged(k, a_in, a_send, a_recv))
    own[...] = jnp.dot(
        compact, a_in[...].reshape(128, 2048), preferred_element_type=jnp.float32
    ).astype(jnp.bfloat16).reshape(own.shape)
    gx[z, core] = own[...]
    each(lambda k: exchange(k, going, a_in, a_send, a_recv).wait_send())

    def at(shift):
        return lax.rem(z + shift + zn, zn)

    def g_copy(direction, hop, e):
        chip = at(-hop if direction == 0 else hop)
        return pltpu.make_async_remote_copy(
            src_ref=own.at[e] if hop == 0 else gx.at[chip, core, e],
            dst_ref=gx.at[chip, core, e],
            send_sem=g_send.at[direction, hop, e], recv_sem=g_recv.at[direction, hop, e],
            device_id=z_up if direction == 0 else z_dn, device_id_type=MESH_ID,
        )

    def g_wait(direction, hop, e):
        chip = at(-hop if direction == 0 else hop)
        pltpu.make_async_remote_copy(
            src_ref=gx.at[chip, core, e], dst_ref=gx.at[chip, core, e],
            send_sem=g_send.at[direction, hop - 1, e], recv_sem=g_recv.at[direction, hop - 1, e],
            device_id=z_up, device_id_type=MESH_ID,
        ).wait_recv()

    def s_copy(shift, e, mine):
        chip = at(shift)
        half = core if mine else 1 - core
        slot = (shift + zn) % zn
        return pltpu.make_async_remote_copy(
            src_ref=own.at[e] if shift == 0 and mine else gx.at[chip, half, e], dst_ref=gx.at[chip, half, e],
            send_sem=s_send.at[slot, e], recv_sem=s_recv.at[slot, e],
            device_id=sib, device_id_type=MESH_ID,
        )

    def x_copy(shift, e):
        chip = at(shift)
        slot = (shift + zn) % zn
        return pltpu.make_async_remote_copy(
            src_ref=py.at[1 - core, chip, e], dst_ref=pd.at[chip, e],
            send_sem=x_send.at[slot, e], recv_sem=x_recv.at[slot, e],
            device_id=sib, device_id_type=MESH_ID,
        )

    for e in (0, 1):
        for direction in (0, 1):
            g_copy(direction, 0, e).start()
    for e in (0, 1):
        s_copy(0, e, True).start()

    def compute(shifts):
        chips = [at(shift) for shift in shifts]

        def one(e, _):
            rows = jnp.concatenate([gx[chip, half, e] for chip in chips for half in (0, 1)], axis=0)
            hidden = jnp.dot(rows, wgu[e], preferred_element_type=jnp.float32)
            gate = jnp.minimum(hidden[:, :256], 7.0)
            up = jnp.clip(hidden[:, 256:], -7.0, 7.0)
            act = ((up + 1.0) * gate * (1.0 / (1.0 + jnp.exp(-1.702 * gate)))).astype(jnp.bfloat16)
            part = jnp.dot(act, wdn[e], preferred_element_type=jnp.float32).astype(jnp.bfloat16)
            for number, chip in enumerate(chips):
                for half in (0, 1):
                    py[half, chip, e] = part[(2 * number + half) * 48:(2 * number + half) * 48 + 48]
            return 0

        lax.fori_loop(0, 2, one, 0)
        for shift in shifts:
            for e in (0, 1):
                x_copy(shift, e).start()

    for load in loads:
        load.wait()
    for e in (0, 1):
        s_copy(0, e, False).wait_recv()
    compute([0])

    def pair_sum(shift, e):
        chip = at(shift)
        return py[core, chip, e].astype(jnp.float32) + pd[chip, e].astype(jnp.float32)

    def r_copy(direction, hop, e):
        return pltpu.make_async_remote_copy(
            src_ref=rs_out.at[direction, hop, e], dst_ref=rs_in.at[direction, hop, e],
            send_sem=r_send.at[direction, hop, e], recv_sem=r_recv.at[direction, hop, e],
            device_id=z_up if direction == 0 else z_dn, device_id_type=MESH_ID,
        )

    seen = set()
    used = []

    def ring(hop, flip):
        for direction in (0, 1):
            e = direction if flip == 0 else 1 - direction
            shift = (far - hop) if direction == 0 else -(far - hop)
            key = (shift % zn, e)
            if key not in seen:
                seen.add(key)
                x_copy(shift, e).wait_recv()
            total = pair_sum(shift, e)
            if hop > 0 and not (hop == 1 and e != direction):
                r_copy(direction, hop - 1, e).wait_recv()
                total = total + rs_in[direction, hop - 1, e].astype(jnp.float32)
            rs_out[direction, hop, e] = total.astype(jnp.bfloat16)
            r_copy(direction, hop, e).start()
            used.append((direction, hop, e))

    for hop in range(1, far + 1):
        if hop == far:
            ring(1, 1)
        for e in (0, 1):
            for direction in (0, 1):
                if hop == far and e != direction:
                    continue
                g_wait(direction, hop, e)
                if hop < far - 1 or (hop == far - 1 and e == direction):
                    g_copy(direction, hop, e).start()
                s_copy(-hop if direction == 0 else hop, e, True).start()
        shifts = [-hop, hop] if hop < far else [far]
        for shift in shifts:
            for e in (0, 1):
                s_copy(shift, e, False).wait_recv()
        compute(shifts)

    for item in ((0, 0), (2, 1), (1, 0), (3, 1), (2, 0), (3, 0)):
        ring(*item)
    sums = []
    for e in (0, 1):
        x_copy(0, e).wait_recv()
        total = pair_sum(0, e)
        for direction in (0, 1):
            r_copy(direction, far - 1, e).wait_recv()
            total = total + rs_in[direction, far - 1, e].astype(jnp.float32)
        sums.append(total.astype(jnp.bfloat16))
    b_out[...] = lax.dot_general(
        compact, jnp.concatenate(sums, axis=0), (((0,), (0,)), ((), ())), preferred_element_type=jnp.float32
    ).astype(jnp.bfloat16).reshape(b_out.shape)
    each(lambda k: exchange(k, b_out, b_in, b_send, b_recv).start())
    b_in[me] = b_out[me]
    each(lambda k: exchanged(k, b_in, b_send, b_recv))
    mixture = jnp.dot(
        mix[...], b_in[...].reshape(128, 2048).astype(jnp.float32),
        preferred_element_type=jnp.float32, precision=lax.Precision.HIGHEST,
    )
    out_ref[...] = (mid[...].astype(jnp.float32) + mixture).astype(jnp.bfloat16)
    each(lambda k: exchange(k, b_out, b_in, b_send, b_recv).wait_send())

    for item in used:
        r_copy(*item).wait_send()
    for e in (0, 1):
        for shift in range(-far + 1, far + 1):
            s_copy(shift, e, True).wait_send()
            x_copy(shift, e).wait_send()
        for direction in (0, 1):
            for hop in range(far):
                if hop < far - 1 or e == direction:
                    g_copy(direction, hop, e).wait_send()


def layer_kernel(*refs):
    ins, weights, out_ref = refs[:17], refs[17:20], refs[20]
    middles, first = refs[21:24], refs[24:24 + A_SCRATCH]
    rest = refs[24 + A_SCRATCH:]
    w_sem, second = rest[0], rest[1:]
    a_in, b_in, wgu, wdn = second[0], second[2], second[7], second[8]
    loads = [
        pltpu.make_async_copy(weights[0], wgu.at[:, :, pl.ds(0, 256)], w_sem.at[0]),
        pltpu.make_async_copy(weights[1], wgu.at[:, :, pl.ds(256, 256)], w_sem.at[1]),
        pltpu.make_async_copy(weights[2], wdn, w_sem.at[2]),
    ]
    for ref in (a_in, b_in):
        ref[...] = jnp.zeros(ref.shape, ref.dtype)
    attend_kernel(loads, *ins, *middles, *first)
    mid, going, mix = middles
    expert_kernel(going, mid, mix, loads, out_ref, *second)


def layer(*args):
    hbm = pl.BlockSpec(memory_space=pltpu.HBM)
    vmem = pl.BlockSpec(memory_space=pltpu.VMEM)
    f32, bf16 = jnp.float32, jnp.bfloat16
    dma = pltpu.SemaphoreType.DMA
    row = pltpu.VMEM((512, 128), f32)
    place = np.arange(512)[:, None]
    first = np.arange(16)[:, None] * 512
    lanes = np.arange(128)[None, :]
    speed = 10000.0 ** (-(lanes % 16) / 16.0)
    live = lanes < ROPE
    base = np.stack([np.cos(place * speed) * live, np.sin(place * speed) * live]).astype(np.float32)
    start = np.stack([np.cos(first * speed) * live, np.sin(first * speed) * live]).astype(np.float32)
    scratch_a = [
            pltpu.VMEM((96, 512), bf16), pltpu.VMEM((160, 512), bf16), pltpu.VMEM((512, 512), bf16),
            pltpu.VMEM((32, 512), bf16), pltpu.VMEM((1, 512), f32),
            pltpu.VMEM((64, 512), bf16), pltpu.VMEM((64, 512), bf16),
            pltpu.VMEM((512, 128), bf16), pltpu.VMEM((512, 128), bf16), pltpu.VMEM((1, 2048), f32),
            pltpu.VMEM((2, 512), jnp.int32), pltpu.VMEM((2, 512), f32),
            pltpu.VMEM((2, 512, 128), f32), pltpu.VMEM((2, 16, 128), f32),
            pltpu.VMEM((2, PIECE, 512), bf16), pltpu.VMEM((512, 256), bf16), pltpu.VMEM((512, 256), bf16),
            pltpu.VMEM((512, 384), bf16),
            pltpu.VMEM((16, 2, PIECE, 512), bf16),
            pltpu.VMEM((256, 2048), bf16),
            pltpu.VMEM((32, 2048), bf16),
            row, row, row, row, row, row,
            pltpu.VMEM((8, 2, 32, 256), bf16),
            pltpu.VMEM((8, 32, 2048), bf16),
            pltpu.VMEM((8, 32, 2048), bf16),
            pltpu.VMEM((8, 32, 2048), bf16),
            pltpu.VMEM((2, 4, 2, 32, 1024), bf16),
            pltpu.VMEM((2, 4, 2, 32, 1024), bf16),
            dma((20,)), dma((20,)), dma((15,)), dma((15,)), dma((17,)),
            dma((8,)), dma((8,)), dma((2, 4, 2)), dma((2, 4, 2)),
        ]
    scratch_b = [
            pltpu.VMEM((16, 8, 2048), bf16), pltpu.VMEM((16, 8, 2048), bf16), pltpu.VMEM((16, 8, 2048), bf16),
            pltpu.VMEM((2, 48, 2048), bf16),
            pltpu.VMEM((8, 2, 2, 48, 2048), bf16),
            pltpu.VMEM((2, 8, 2, 48, 2048), bf16),
            pltpu.VMEM((8, 2, 48, 2048), bf16),
            pltpu.VMEM((2, 2048, 512), bf16),
            pltpu.VMEM((2, 256, 2048), bf16),
            pltpu.VMEM((2, 4, 2, 48, 2048), bf16),
            pltpu.VMEM((2, 4, 2, 48, 2048), bf16),
            dma((16,)), dma((16,)), dma((16,)), dma((16,)),
            dma((2, 4, 2)), dma((2, 4, 2)), dma((8, 2)), dma((8, 2)),
            dma((8, 2)), dma((8, 2)), dma((2, 4, 2)), dma((2, 4, 2)),
        ]
    assert len(scratch_a) == A_SCRATCH
    return pl.pallas_call(
        layer_kernel,
        out_shape=jax.ShapeDtypeStruct((32, 2048), bf16),
        in_specs=[hbm] * 20,
        out_specs=vmem,
        scratch_shapes=[
            pltpu.VMEM((32, 2048), bf16), pltpu.VMEM((16, 8, 2048), bf16), pltpu.VMEM((32, 128), f32),
            *scratch_a, dma((3,)), *scratch_b,
        ],
        compiler_params=pltpu.CompilerParams(collective_id=1, has_side_effects=True, vmem_limit_bytes=67043328),
        name="gather_attend_experts",
    )(*args[:15], jnp.asarray(base), jnp.asarray(start), *args[15:])


def body(
    query_first, query_second, latent, key_rotary, latent_gain, key_up_first, value_up_first,
    key_up_second, value_up_second, out_first, out_second, residual, expert_gain,
    route_experts, route_scores, gate_weight, up_weight, down_weight,
):
    return layer(
        query_first.T, query_second.T, latent, key_rotary.T, latent_gain.reshape(1, -1), key_up_first.T, value_up_first.T,
        key_up_second, value_up_second, out_first, out_second, residual, expert_gain.reshape(1, -1),
        route_experts.T, route_scores.T, gate_weight, up_weight, down_weight,
    )


def solution(mesh):
    in_specs = (
        P("sp", "tp"), P("sp", "tp"), P("sp", None), P("sp", None), P(),
        P(None, "tp"), P(None, "tp"), P(None, "tp"), P(None, "tp"),
        P("tp", None), P("tp", None), P("sp", None), P(),
        P("sp", None), P("sp", None), P("sp", None, "tp"), P("sp", None, "tp"), P("sp", "tp", None),
    )
    out_specs = P(("sp", "tp"), None)
    return jax.shard_map(body, mesh=mesh, in_specs=in_specs, out_specs=out_specs, check_vma=False)
```

```python
import jax
import jax.numpy as jnp
import numpy as np
from jax import lax
from jax.experimental import pallas as pl
from jax.experimental.pallas import tpu as pltpu
from jax.sharding import PartitionSpec as P

NA, NB, ROPE, CAP = 64, 128, 32, 3
EPS = 1e-6
MASKED = -1e30
LOG2E = 1.4426950408889634
SIDE = 4
HALF_ROWS = 256
KT_ROWS = 16
PIECE = HALF_ROWS + KT_ROWS
A_SCRATCH = 42
CUT = 144
MESH_ID = pl.DeviceIdType.MESH
STEPS = (
    (-1, 0), (1, 0), (0, -1), (0, 1), (2, 0), (-1, -1), (-1, 1), (1, -1), (1, 1),
    (0, 2), (2, -1), (2, 1), (-1, 2), (1, 2), (2, 2),
)


def pick(index, values):
    out = jnp.int32(values[0])
    for at, value in enumerate(values):
        if at:
            out = jnp.where(index == at, jnp.int32(value), out)
    return out


def attend_kernel(
    weight_loads, qf_hbm, qs_hbm, lat_hbm, kr_hbm, latg_hbm, kuf_hbm, vuf_hbm, kus_hbm, vus_hbm,
    of_hbm, os_hbm, res_hbm, gain_hbm, ids_hbm, scores_hbm, base_hbm, start_hbm,
    mid_ref, out_ref, mix_ref,
    qf, qs, lat, kr, latg, kuf, vuf, kus, vus, gain, ids, scores, base, start,
    own, q1, q2, wup,
    buf, wout, res, m1, l1, o1, m2, l2, o2, att, po, px, pd, rs_out, rs_in,
    g_send, g_recv, d_send, d_recv, loc_sem, x_send, x_recv, r_send, r_recv,
):
    me = lax.axis_index("sp")
    tp = lax.axis_index("tp")
    core = lax.rem(tp, 2)
    z = lax.div(tp, 2)
    y = lax.div(me, SIDE)
    x = lax.rem(me, SIDE)
    zn = lax.axis_size("tp") // 2

    def block(c, dp, dq):
        p = lax.rem(x + c * (y - x) + dp + SIDE, SIDE)
        q = lax.rem(y + c * (x - y) + dq + SIDE, SIDE)
        return p * (1 + 3 * c) + q * (4 - 3 * c)

    def sp_dev(dp, dq):
        return {"sp": block(core, dp, dq), "tp": tp}

    sib = {"sp": me, "tp": tp + 1 - 2 * core}
    z_up = {"sp": me, "tp": lax.rem(z + 1, zn) * 2 + core}
    z_dn = {"sp": me, "tp": lax.rem(z + zn - 1, zn) * 2 + core}
    groups = lax.axis_size("sp")
    peers = [sib, z_up, z_dn] + [{"sp": lax.rem(me + k, groups), "tp": tp} for k in range(1, groups)]

    mine = pl.ds(pl.multiple_of(tp * 32, 32), 32)
    pairs = [
        (lat_hbm, lat), (latg_hbm, latg), (kr_hbm, kr), (base_hbm, base), (start_hbm, start),
        (qf_hbm, qf), (qs_hbm, qs), (kus_hbm, kus), (kuf_hbm, kuf), (vuf_hbm, vuf), (vus_hbm, vus),
        (of_hbm, wout.at[pl.ds(64, 64)]), (os_hbm, wout.at[pl.ds(128, 128)]), (res_hbm.at[mine], res),
        (gain_hbm, gain), (ids_hbm, ids), (scores_hbm, scores),
    ]
    loads = [pltpu.make_async_copy(a, b, loc_sem.at[n]) for n, (a, b) in enumerate(pairs)]
    for load in loads + weight_loads:
        load.start()
    wout[pl.ds(0, 64)] = jnp.zeros((64, wout.shape[1]), wout.dtype)
    m1[...] = jnp.full(m1.shape, MASKED, jnp.float32)
    m2[...] = jnp.full(m2.shape, MASKED, jnp.float32)
    for ref in (l1, o1, l2, o2):
        ref[...] = jnp.zeros(ref.shape, jnp.float32)

    barrier = pltpu.get_barrier_semaphore()
    for peer in peers:
        pl.semaphore_signal(barrier, inc=1, device_id=peer, device_id_type=MESH_ID)

    f32, bf16 = jnp.float32, jnp.bfloat16

    def placed(rows, cols, hits):
        r = lax.broadcasted_iota(jnp.int32, (rows, cols), 0)
        c = lax.broadcasted_iota(jnp.int32, (rows, cols), 1)
        total = jnp.zeros((rows, cols), f32)
        for lo, hi, shift, sign in hits:
            total = jnp.where((r == c + shift) & (c >= lo) & (c < hi), sign, total)
        return total.astype(bf16)

    def moved(value, cols, hits):
        return lax.dot_general(
            value, placed(value.shape[0], cols, hits), (((0,), (0,)), ((), ())), preferred_element_type=f32
        )

    for load in loads[:5]:
        load.wait()
    cos_r, sin_r = base[0], base[1]
    cos_0, sin_0 = start[0, pl.ds(me, 1)], start[1, pl.ds(me, 1)]
    cosine = cos_0 * cos_r - sin_0 * sin_r
    sine = sin_0 * cos_r + cos_0 * sin_r

    def rot(value, offset):
        plain = moved(value, 128, [(0, 32, offset, 1.0)])
        crossed = moved(value, 128, [(0, 16, offset + 16, -1.0), (16, 32, offset - 16, 1.0)])
        return (plain * cosine + crossed * sine).astype(bf16)

    wide = lat[...].astype(f32)
    normed = (wide * lax.rsqrt(jnp.mean(wide * wide, axis=1, keepdims=True) + EPS) * latg[...]).astype(bf16)
    own[:, pl.ds(KT_ROWS, HALF_ROWS)] = normed.reshape(2, HALF_ROWS, 512)
    kt = rot(kr[...], 0).astype(f32)
    rolled = [kt] + [pltpu.roll(kt, 32 * j, 1) for j in (1, 2, 3)]
    for half in (0, 1):
        tiles = []
        for tile in range(4):
            total = 0.0
            for j in range(4):
                first = half * HALF_ROWS + (4 * tile + j) * 16
                total = total + rolled[j][first:first + 16]
            tiles.append(total)
        own[half, pl.ds(0, KT_ROWS)] = jnp.concatenate(tiles, axis=1).astype(bf16)
    pl.semaphore_wait(barrier, len(peers))

    A, B, FULL = (0, CUT), (CUT, PIECE - CUT), (0, PIECE)

    def g_copy(sem, off, rows, dev, src_own=False):
        b = block(core, *off)
        src = own.at[core, pl.ds(rows[0], rows[1])] if src_own else buf.at[b, core, pl.ds(rows[0], rows[1])]
        return pltpu.make_async_remote_copy(
            src_ref=src, dst_ref=buf.at[b, core, pl.ds(rows[0], rows[1])],
            send_sem=g_send.at[sem], recv_sem=g_recv.at[sem],
            device_id=dev, device_id_type=MESH_ID,
        )

    right, left, up, down = sp_dev(1, 0), sp_dev(-1, 0), sp_dev(0, 1), sp_dev(0, -1)
    X, L, R, O = (0, 0), (-1, 0), (1, 0), (2, 0)
    sends = {
        0: (X, FULL, right, True), 1: (X, FULL, left, True), 2: (X, FULL, up, True), 3: (X, FULL, down, True),
        4: (L, A, right, False), 5: (R, B, left, False),
        6: (L, FULL, up, False), 7: (L, FULL, down, False), 8: (R, FULL, up, False), 9: (R, FULL, down, False),
        10: (O, FULL, up, False), 11: (O, FULL, down, False),
    }
    for k, dp in enumerate((0, -1, 1, 2)):
        sends[12 + 2 * k] = ((dp, -1), A, up, False)
        sends[13 + 2 * k] = ((dp, 1), B, down, False)
    arrive = {0: (L, FULL), 1: (R, FULL), 2: ((0, -1), FULL), 3: ((0, 1), FULL), 4: (O, A), 5: (O, B)}
    for k, dp in enumerate((0, -1, 1, 2)):
        if k:
            arrive[4 + 2 * k] = ((dp, -1), FULL)
            arrive[5 + 2 * k] = ((dp, 1), FULL)
        arrive[12 + 2 * k] = ((dp, 2), A)
        arrive[13 + 2 * k] = ((dp, 2), B)

    def send(sem):
        off, rows, dev, src_own = sends[sem]
        g_copy(sem, off, rows, dev, src_own).start()

    def arrived(sem):
        off, rows = arrive[sem]
        g_copy(sem, off, rows, right).wait_recv()

    def d_copy(event, blk, half):
        return pltpu.make_async_remote_copy(
            src_ref=buf.at[blk, half], dst_ref=buf.at[blk, half],
            send_sem=d_send.at[event], recv_sem=d_recv.at[event],
            device_id=sib, device_id_type=MESH_ID,
        )

    events = [
        ((0,), (4, 6, 7)), ((1,), (5, 8, 9)), ((2,), (12,)), ((3,), (13,)), ((4, 5), (10, 11)),
        ((6,), (14,)), ((7,), (15,)), ((8,), (16,)), ((9,), (17,)),
        ((12, 13), ()), ((10,), (18,)), ((11,), (19,)), ((14, 15), ()), ((16, 17), ()), ((18, 19), ()),
    ]

    for sem in (0, 1, 2, 3):
        send(sem)

    c1 = LOG2E * (NA + ROPE) ** -0.5
    c2 = LOG2E * (NB + ROPE) ** -0.5
    for load in loads[5:]:
        load.wait()
    q1[:, pl.ds(0, 128)] = moved(qf[...], 128, [(0, 64, 0, 1.0)]).astype(bf16)
    q1[:, pl.ds(128, 128)] = rot(qf[...], NA)
    q2[:, pl.ds(0, 128)] = moved(qs[...], 128, [(0, 128, 0, 1.0)]).astype(bf16)
    q2[:, pl.ds(128, 128)] = rot(qs[...], NB)
    wup[:, pl.ds(0, 128)] = kus[...]
    wup[:, pl.ds(128, 128)] = (moved(kuf[...], 128, [(0, 64, 0, 1.0)]) + moved(vuf[...], 128, [(64, 128, -64, 1.0)])).astype(bf16)
    wup[:, pl.ds(256, 128)] = vus[...]

    def unpack_turned(packed):
        wide = packed.astype(jnp.float32)
        rolled = [wide] + [pltpu.roll(wide, 512 - 32 * j, 1) for j in (1, 2, 3)]
        parts = [rolled[k % 4][:, (k // 4) * 128:(k // 4) * 128 + 128] for k in range(16)]
        return jnp.concatenate(parts, axis=0).astype(jnp.bfloat16)

    def head(q, keys, values, m, l, o, scale, masked):
        s = lax.dot_general(q[...], keys, (((1,), (1,)), ((), ())), preferred_element_type=jnp.float32)
        if masked is not None:
            s = jnp.where(masked, s, MASKED)
        old = m[...]
        new = jnp.maximum(old, jnp.max(s, axis=1, keepdims=True))
        m[...] = new
        fade = jnp.exp2((old - new) * scale)
        p = jnp.exp2((s - jnp.concatenate([new, new], axis=1)) * scale)
        l[...] = l[...] * fade + (p[:, :128] + p[:, 128:])
        o[...] = o[...] * fade + jnp.dot(p.astype(jnp.bfloat16), values, preferred_element_type=jnp.float32)

    def compute(piece, masked):
        turned = unpack_turned(piece[pl.ds(0, KT_ROWS)])
        kv = jnp.dot(piece[pl.ds(KT_ROWS, HALF_ROWS)], wup[...], preferred_element_type=jnp.float32).astype(jnp.bfloat16)
        kfv = kv[:, 128:256]
        head(q1, jnp.concatenate([kfv, turned], axis=1), kfv, m1, l1, o1, c1, masked)
        head(q2, jnp.concatenate([kv[:, :128], turned], axis=1), kv[:, 256:384], m2, l2, o2, c2, masked)

    def diag(half, _):
        rows = lax.broadcasted_iota(jnp.int32, (2 * HALF_ROWS, HALF_ROWS), 0)
        cols = lax.broadcasted_iota(jnp.int32, (2 * HALF_ROWS, HALF_ROWS), 1) + half * HALF_ROWS
        compute(own.at[half], rows >= cols)
        return 0

    lax.fori_loop(0, 2, diag, 0)

    count = len(events)

    def step(it, _):
        theirs = lax.rem(it, 2)
        event = lax.div(it, 2) - theirs
        stream = core + theirs * (1 - 2 * core)
        blk = block(stream, pick(event, [s[0] for s in STEPS]), pick(event, [s[1] for s in STEPS]))

        for number, (waits, starts) in enumerate(events):
            @pl.when(it == 2 * number)
            def _():
                for sem in waits:
                    arrived(sem)
                for sem in starts:
                    send(sem)

        @pl.when((theirs == 0) & (event < count))
        def _():
            d_copy(event, blk, core).start()

        @pl.when((theirs == 1) & (event >= 0))
        def _():
            d_copy(event, blk, 1 - core).wait_recv()

        @pl.when((blk < me) & (event >= 0) & (event < count))
        def _():
            compute(buf.at[blk, stream], None)

        return 0

    lax.fori_loop(0, 2 * count + 2, step, 0)

    for sem in range(20):
        off, rows, dev, src_own = sends[sem]
        g_copy(sem, off, rows, dev, src_own).wait_send()

    def drain(event, _):
        d_copy(event, block(core, pick(event, [s[0] for s in STEPS]), pick(event, [s[1] for s in STEPS])), core).wait_send()
        return 0

    lax.fori_loop(0, count, drain, 0)

    a1 = o1[...] / jnp.sum(l1[...], axis=1, keepdims=True)
    a2 = o2[...] / jnp.sum(l2[...], axis=1, keepdims=True)
    lane = lax.broadcasted_iota(jnp.int32, a1.shape, 1)
    a1 = jnp.where(lane >= 64, a1, 0.0)
    both = jnp.concatenate([a1, a2], axis=1).astype(jnp.bfloat16)
    att[...] = both.reshape(att.shape)


    def project(c, into):
        rows = att[:, pl.ds(c, 1)].reshape(zn * 32, 256)
        into[...] = jnp.dot(rows, wout[...], preferred_element_type=jnp.float32).astype(jnp.bfloat16).reshape(into.shape)

    def x_copy(d):
        at = lax.rem(z + d, zn)
        return pltpu.make_async_remote_copy(
            src_ref=px.at[at], dst_ref=pd.at[at], send_sem=x_send.at[d], recv_sem=x_recv.at[d],
            device_id=sib, device_id_type=MESH_ID,
        )

    far = zn // 2
    order = [far]
    for d in range(far - 1, 0, -1):
        order += [d, zn - d]
    order.append(0)
    project(1 - core, px)
    for d in order:
        x_copy(d).start()
    project(core, po)

    width = 512
    native = ((0, 1), (2, 3))

    def pair_sum(at, col, width):
        return po[at, :, pl.ds(col, width)].astype(jnp.float32) + pd[at, :, pl.ds(col, width)].astype(jnp.float32)

    def r_copy(direction, hop, part):
        return pltpu.make_async_remote_copy(
            src_ref=rs_out.at[direction, hop, part], dst_ref=rs_in.at[direction, hop, part],
            send_sem=r_send.at[direction, hop, part], recv_sem=r_recv.at[direction, hop, part],
            device_id=z_up if direction == 0 else z_dn, device_id_type=MESH_ID,
        )

    seen = set()

    def ring(direction, hop, part):
        d = far - hop
        shift = d if direction == 0 else (zn - d) % zn
        if shift not in seen:
            x_copy(shift).wait_recv()
            seen.add(shift)
        total = pair_sum(lax.rem(z + shift, zn), part * width, width)
        if hop > 0 and not (hop == 1 and part not in native[direction]):
            r_copy(direction, hop - 1, part).wait_recv()
            total = total + rs_in[direction, hop - 1, part].astype(jnp.float32)
        rs_out[direction, hop, part] = total.astype(jnp.bfloat16)
        r_copy(direction, hop, part).start()

    used = []
    for hop, flip in ((0, 0), (1, 1), (1, 0), (2, 1), (2, 0), (3, 1), (3, 0)):
        for which in (0, 1):
            for direction in (0, 1):
                part = native[direction ^ flip][which]
                ring(direction, hop, part)
                used.append((direction, hop, part))
    x_copy(0).wait_recv()
    mids = []
    for part in (0, 2, 1, 3):
        total = pair_sum(z, part * width, width)
        for direction in (0, 1):
            r_copy(direction, far - 1, part).wait_recv()
            total = total + rs_in[direction, far - 1, part].astype(jnp.float32)
        mids.append((res[:, pl.ds(part * width, width)].astype(jnp.float32) + total).astype(jnp.bfloat16))
    mid = jnp.concatenate([mids[0], mids[2], mids[1], mids[3]], axis=1)
    mid_ref[...] = mid
    wide = mid.astype(jnp.float32)
    normed = (wide * lax.rsqrt(jnp.mean(wide * wide, axis=1, keepdims=True) + EPS) * gain[...]).astype(bf16)
    slots = mix_ref.shape[1]
    token = lax.broadcasted_iota(jnp.int32, (32, 512), 1) == lax.broadcasted_iota(jnp.int32, (32, 512), 0) + tp * 32
    names = [jnp.sum(jnp.where(token, ids[k:k + 1], 0), axis=1, keepdims=True) for k in (0, 1)]
    logits = [jnp.sum(jnp.where(token, scores[k:k + 1], 0.0), axis=1, keepdims=True) for k in (0, 1)]
    hits = [(lax.broadcasted_iota(jnp.int32, (32, 128), 1) == name).astype(f32) for name in names]
    earlier = lax.broadcasted_iota(jnp.int32, (32, 32), 0) > lax.broadcasted_iota(jnp.int32, (32, 32), 1)
    before = jnp.dot(earlier.astype(bf16), (hits[0] + hits[1]).astype(bf16), preferred_element_type=f32)
    top = jnp.maximum(logits[0], logits[1])
    powers = [jnp.exp(logit - top) for logit in logits]
    picked, mix = 0.0, 0.0
    for k in (0, 1):
        rank = jnp.sum(before * hits[k], axis=1, keepdims=True)
        slot = (names[k] >> 1) * 8 + (names[k] & 1) * CAP + rank.astype(jnp.int32)
        here = (lax.broadcasted_iota(jnp.int32, (32, slots), 1) == slot).astype(f32)
        picked = picked + here
        mix = mix + here * (powers[k] / (powers[0] + powers[1]))
    mix_ref[...] = mix
    out_ref[...] = lax.dot_general(
        picked.astype(bf16), normed, (((0,), (0,)), ((), ())), preferred_element_type=f32
    ).astype(bf16).reshape(out_ref.shape)
    for d in order:
        x_copy(d).wait_send()
    for item in used:
        r_copy(*item).wait_send()


def expert_kernel(
    going, mid, mix, loads, out_ref,
    a_in, b_out, b_in, own, gx, py, pd, wgu, wdn, rs_out, rs_in,
    a_send, a_recv, b_send, b_recv, g_send, g_recv, s_send, s_recv, x_send, x_recv, r_send, r_recv,
):
    me = lax.axis_index("sp")
    tp = lax.axis_index("tp")
    core = lax.rem(tp, 2)
    z = lax.div(tp, 2)
    zn = lax.axis_size("tp") // 2
    far = zn // 2
    sib = {"sp": me, "tp": tp + 1 - 2 * core}
    z_up = {"sp": me, "tp": lax.rem(z + 1, zn) * 2 + core}
    z_dn = {"sp": me, "tp": lax.rem(z + zn - 1, zn) * 2 + core}
    groups = lax.axis_size("sp")

    def exchange(k, src, dst, send_sems, recv_sems):
        peer = lax.rem(me + k, groups)
        return pltpu.make_async_remote_copy(
            src_ref=src.at[peer, pl.ds(0, 6)], dst_ref=dst.at[me, pl.ds(0, 6)], send_sem=send_sems.at[k], recv_sem=recv_sems.at[k],
            device_id={"sp": peer, "tp": tp}, device_id_type=MESH_ID,
        )

    def exchanged(k, dst, send_sems, recv_sems):
        peer = lax.rem(me + groups - k, groups)
        pltpu.make_async_remote_copy(
            src_ref=dst.at[peer, pl.ds(0, 6)], dst_ref=dst.at[peer, pl.ds(0, 6)], send_sem=send_sems.at[k], recv_sem=recv_sems.at[k],
            device_id={"sp": peer, "tp": tp}, device_id_type=MESH_ID,
        ).wait_recv()

    def each(act):
        def one(k, _):
            act(k)
            return 0

        lax.fori_loop(1, groups, one, 0)

    each(lambda k: exchange(k, going, a_in, a_send, a_recv).start())
    a_in[me] = going[me]
    row = lax.broadcasted_iota(jnp.int32, (96, 128), 0)
    col = lax.broadcasted_iota(jnp.int32, (96, 128), 1)
    inner = col & 7
    second = (inner >= CAP).astype(jnp.int32)
    wanted = second * 48 + (col >> 3) * CAP + inner - second * CAP
    compact = ((row == wanted) & (inner < 2 * CAP)).astype(jnp.float32).astype(jnp.bfloat16)
    each(lambda k: exchanged(k, a_in, a_send, a_recv))
    own[...] = jnp.dot(
        compact, a_in[...].reshape(128, 2048), preferred_element_type=jnp.float32
    ).astype(jnp.bfloat16).reshape(own.shape)
    gx[z, core] = own[...]
    each(lambda k: exchange(k, going, a_in, a_send, a_recv).wait_send())

    def at(shift):
        return lax.rem(z + shift + zn, zn)

    def g_copy(direction, hop, e):
        chip = at(-hop if direction == 0 else hop)
        return pltpu.make_async_remote_copy(
            src_ref=own.at[e] if hop == 0 else gx.at[chip, core, e],
            dst_ref=gx.at[chip, core, e],
            send_sem=g_send.at[direction, hop, e], recv_sem=g_recv.at[direction, hop, e],
            device_id=z_up if direction == 0 else z_dn, device_id_type=MESH_ID,
        )

    def g_wait(direction, hop, e):
        chip = at(-hop if direction == 0 else hop)
        pltpu.make_async_remote_copy(
            src_ref=gx.at[chip, core, e], dst_ref=gx.at[chip, core, e],
            send_sem=g_send.at[direction, hop - 1, e], recv_sem=g_recv.at[direction, hop - 1, e],
            device_id=z_up, device_id_type=MESH_ID,
        ).wait_recv()

    def s_copy(shift, e, mine):
        chip = at(shift)
        half = core if mine else 1 - core
        slot = (shift + zn) % zn
        return pltpu.make_async_remote_copy(
            src_ref=own.at[e] if shift == 0 and mine else gx.at[chip, half, e], dst_ref=gx.at[chip, half, e],
            send_sem=s_send.at[slot, e], recv_sem=s_recv.at[slot, e],
            device_id=sib, device_id_type=MESH_ID,
        )

    def x_copy(shift, e):
        chip = at(shift)
        slot = (shift + zn) % zn
        return pltpu.make_async_remote_copy(
            src_ref=py.at[1 - core, chip, e], dst_ref=pd.at[chip, e],
            send_sem=x_send.at[slot, e], recv_sem=x_recv.at[slot, e],
            device_id=sib, device_id_type=MESH_ID,
        )

    for e in (0, 1):
        for direction in (0, 1):
            g_copy(direction, 0, e).start()
    for e in (0, 1):
        s_copy(0, e, True).start()

    def compute(shifts):
        chips = [at(shift) for shift in shifts]

        def one(e, _):
            rows = jnp.concatenate([gx[chip, half, e] for chip in chips for half in (0, 1)], axis=0)
            hidden = jnp.dot(rows, wgu[e], preferred_element_type=jnp.float32)
            gate = jnp.minimum(hidden[:, :256], 7.0)
            up = jnp.clip(hidden[:, 256:], -7.0, 7.0)
            act = ((up + 1.0) * gate * (1.0 / (1.0 + jnp.exp(-1.702 * gate)))).astype(jnp.bfloat16)
            part = jnp.dot(act, wdn[e], preferred_element_type=jnp.float32).astype(jnp.bfloat16)
            for number, chip in enumerate(chips):
                for half in (0, 1):
                    py[half, chip, e] = part[(2 * number + half) * 48:(2 * number + half) * 48 + 48]
            return 0

        lax.fori_loop(0, 2, one, 0)
        for shift in shifts:
            for e in (0, 1):
                x_copy(shift, e).start()

    for load in loads:
        load.wait()
    for e in (0, 1):
        s_copy(0, e, False).wait_recv()
    compute([0])

    def pair_sum(shift, e):
        chip = at(shift)
        return py[core, chip, e].astype(jnp.float32) + pd[chip, e].astype(jnp.float32)

    def r_copy(direction, hop, e):
        return pltpu.make_async_remote_copy(
            src_ref=rs_out.at[direction, hop, e], dst_ref=rs_in.at[direction, hop, e],
            send_sem=r_send.at[direction, hop, e], recv_sem=r_recv.at[direction, hop, e],
            device_id=z_up if direction == 0 else z_dn, device_id_type=MESH_ID,
        )

    seen = set()
    used = []

    def ring(hop, flip):
        for direction in (0, 1):
            e = direction if flip == 0 else 1 - direction
            shift = (far - hop) if direction == 0 else -(far - hop)
            key = (shift % zn, e)
            if key not in seen:
                seen.add(key)
                x_copy(shift, e).wait_recv()
            total = pair_sum(shift, e)
            if hop > 0 and not (hop == 1 and e != direction):
                r_copy(direction, hop - 1, e).wait_recv()
                total = total + rs_in[direction, hop - 1, e].astype(jnp.float32)
            rs_out[direction, hop, e] = total.astype(jnp.bfloat16)
            r_copy(direction, hop, e).start()
            used.append((direction, hop, e))

    for hop in range(1, far + 1):
        if hop == far:
            ring(1, 1)
        for e in (0, 1):
            for direction in (0, 1):
                if hop == far and e != direction:
                    continue
                g_wait(direction, hop, e)
                if hop < far - 1 or (hop == far - 1 and e == direction):
                    g_copy(direction, hop, e).start()
                s_copy(-hop if direction == 0 else hop, e, True).start()
        shifts = [-hop, hop] if hop < far else [far]
        for shift in shifts:
            for e in (0, 1):
                s_copy(shift, e, False).wait_recv()
        compute(shifts)

    for item in ((0, 0), (2, 1), (1, 0), (3, 1), (2, 0), (3, 0)):
        ring(*item)
    sums = []
    for e in (0, 1):
        x_copy(0, e).wait_recv()
        total = pair_sum(0, e)
        for direction in (0, 1):
            r_copy(direction, far - 1, e).wait_recv()
            total = total + rs_in[direction, far - 1, e].astype(jnp.float32)
        sums.append(total.astype(jnp.bfloat16))
    b_out[...] = lax.dot_general(
        compact, jnp.concatenate(sums, axis=0), (((0,), (0,)), ((), ())), preferred_element_type=jnp.float32
    ).astype(jnp.bfloat16).reshape(b_out.shape)
    each(lambda k: exchange(k, b_out, b_in, b_send, b_recv).start())
    b_in[me] = b_out[me]
    each(lambda k: exchanged(k, b_in, b_send, b_recv))
    mixture = jnp.dot(
        mix[...], b_in[...].reshape(128, 2048).astype(jnp.float32),
        preferred_element_type=jnp.float32, precision=lax.Precision.HIGHEST,
    )
    out_ref[...] = (mid[...].astype(jnp.float32) + mixture).astype(jnp.bfloat16)
    each(lambda k: exchange(k, b_out, b_in, b_send, b_recv).wait_send())

    for item in used:
        r_copy(*item).wait_send()
    for e in (0, 1):
        for shift in range(-far + 1, far + 1):
            s_copy(shift, e, True).wait_send()
            x_copy(shift, e).wait_send()
        for direction in (0, 1):
            for hop in range(far):
                if hop < far - 1 or e == direction:
                    g_copy(direction, hop, e).wait_send()


def layer_kernel(*refs):
    ins, weights, out_ref = refs[:17], refs[17:20], refs[20]
    middles, first = refs[21:24], refs[24:24 + A_SCRATCH]
    rest = refs[24 + A_SCRATCH:]
    w_sem, second = rest[0], rest[1:]
    a_in, b_in, wgu, wdn = second[0], second[2], second[7], second[8]
    loads = [
        pltpu.make_async_copy(weights[0], wgu.at[:, :, pl.ds(0, 256)], w_sem.at[0]),
        pltpu.make_async_copy(weights[1], wgu.at[:, :, pl.ds(256, 256)], w_sem.at[1]),
        pltpu.make_async_copy(weights[2], wdn, w_sem.at[2]),
    ]
    for ref in (a_in, b_in):
        ref[...] = jnp.zeros(ref.shape, ref.dtype)
    attend_kernel(loads, *ins, *middles, *first)
    mid, going, mix = middles
    expert_kernel(going, mid, mix, loads, out_ref, *second)


def layer(*args):
    hbm = pl.BlockSpec(memory_space=pltpu.HBM)
    vmem = pl.BlockSpec(memory_space=pltpu.VMEM)
    f32, bf16 = jnp.float32, jnp.bfloat16
    dma = pltpu.SemaphoreType.DMA
    row = pltpu.VMEM((512, 128), f32)
    place = np.arange(512)[:, None]
    first = np.arange(16)[:, None] * 512
    lanes = np.arange(128)[None, :]
    speed = 10000.0 ** (-(lanes % 16) / 16.0)
    live = lanes < ROPE
    base = np.stack([np.cos(place * speed) * live, np.sin(place * speed) * live]).astype(np.float32)
    start = np.stack([np.cos(first * speed) * live, np.sin(first * speed) * live]).astype(np.float32)
    scratch_a = [
            pltpu.VMEM((96, 512), bf16), pltpu.VMEM((160, 512), bf16), pltpu.VMEM((512, 512), bf16),
            pltpu.VMEM((32, 512), bf16), pltpu.VMEM((1, 512), f32),
            pltpu.VMEM((64, 512), bf16), pltpu.VMEM((64, 512), bf16),
            pltpu.VMEM((512, 128), bf16), pltpu.VMEM((512, 128), bf16), pltpu.VMEM((1, 2048), f32),
            pltpu.VMEM((2, 512), jnp.int32), pltpu.VMEM((2, 512), f32),
            pltpu.VMEM((2, 512, 128), f32), pltpu.VMEM((2, 16, 128), f32),
            pltpu.VMEM((2, PIECE, 512), bf16), pltpu.VMEM((512, 256), bf16), pltpu.VMEM((512, 256), bf16),
            pltpu.VMEM((512, 384), bf16),
            pltpu.VMEM((16, 2, PIECE, 512), bf16),
            pltpu.VMEM((256, 2048), bf16),
            pltpu.VMEM((32, 2048), bf16),
            row, row, row, row, row, row,
            pltpu.VMEM((8, 2, 32, 256), bf16),
            pltpu.VMEM((8, 32, 2048), bf16),
            pltpu.VMEM((8, 32, 2048), bf16),
            pltpu.VMEM((8, 32, 2048), bf16),
            pltpu.VMEM((2, 4, 4, 32, 512), bf16),
            pltpu.VMEM((2, 4, 4, 32, 512), bf16),
            dma((20,)), dma((20,)), dma((15,)), dma((15,)), dma((17,)),
            dma((8,)), dma((8,)), dma((2, 4, 4)), dma((2, 4, 4)),
        ]
    scratch_b = [
            pltpu.VMEM((16, 8, 2048), bf16), pltpu.VMEM((16, 8, 2048), bf16), pltpu.VMEM((16, 8, 2048), bf16),
            pltpu.VMEM((2, 48, 2048), bf16),
            pltpu.VMEM((8, 2, 2, 48, 2048), bf16),
            pltpu.VMEM((2, 8, 2, 48, 2048), bf16),
            pltpu.VMEM((8, 2, 48, 2048), bf16),
            pltpu.VMEM((2, 2048, 512), bf16),
            pltpu.VMEM((2, 256, 2048), bf16),
            pltpu.VMEM((2, 4, 2, 48, 2048), bf16),
            pltpu.VMEM((2, 4, 2, 48, 2048), bf16),
            dma((16,)), dma((16,)), dma((16,)), dma((16,)),
            dma((2, 4, 2)), dma((2, 4, 2)), dma((8, 2)), dma((8, 2)),
            dma((8, 2)), dma((8, 2)), dma((2, 4, 2)), dma((2, 4, 2)),
        ]
    assert len(scratch_a) == A_SCRATCH
    return pl.pallas_call(
        layer_kernel,
        out_shape=jax.ShapeDtypeStruct((32, 2048), bf16),
        in_specs=[hbm] * 20,
        out_specs=vmem,
        scratch_shapes=[
            pltpu.VMEM((32, 2048), bf16), pltpu.VMEM((16, 8, 2048), bf16), pltpu.VMEM((32, 128), f32),
            *scratch_a, dma((3,)), *scratch_b,
        ],
        compiler_params=pltpu.CompilerParams(collective_id=1, has_side_effects=True, vmem_limit_bytes=67043328),
        name="gather_attend_experts",
    )(*args[:15], jnp.asarray(base), jnp.asarray(start), *args[15:])


def body(
    query_first, query_second, latent, key_rotary, latent_gain, key_up_first, value_up_first,
    key_up_second, value_up_second, out_first, out_second, residual, expert_gain,
    route_experts, route_scores, gate_weight, up_weight, down_weight,
):
    return layer(
        query_first.T, query_second.T, latent, key_rotary.T, latent_gain.reshape(1, -1), key_up_first.T, value_up_first.T,
        key_up_second, value_up_second, out_first, out_second, residual, expert_gain.reshape(1, -1),
        route_experts.T, route_scores.T, gate_weight, up_weight, down_weight,
    )


def solution(mesh):
    in_specs = (
        P("sp", "tp"), P("sp", "tp"), P("sp", None), P("sp", None), P(),
        P(None, "tp"), P(None, "tp"), P(None, "tp"), P(None, "tp"),
        P("tp", None), P("tp", None), P("sp", None), P(),
        P("sp", None), P("sp", None), P("sp", None, "tp"), P("sp", None, "tp"), P("sp", "tp", None),
    )
    out_specs = P(("sp", "tp"), None)
    return jax.shard_map(body, mesh=mesh, in_specs=in_specs, out_specs=out_specs, check_vma=False)
```
